256 devices in a mesh: ep: 64 (over z, y, core), tp: 4 (over x).
Axes of the slice: x: 4, y: 4, z: 8, core: 2. Of those that a mesh axis runs over, the one named last changes fastest.
Arguments:
- queries: bfloat16 [65536, 1024], P('ep', 'tp'), may hold values from -6 to 6
- head_keys: bfloat16 [65536, 256], P('ep', 'tp'), may hold values from -6 to 6
- head_values: bfloat16 [65536, 256], P('ep', 'tp'), may hold values from -6 to 6
- sink_logits: float32 [16], P('tp'), may hold values from -2 to 5
- out_weight: bfloat16 [1024, 2048], P('tp'), may hold values from -1.5 to 1.5
- moe_input: bfloat16 [32768, 2048], P(('ep', 'tp')), may hold values from -6 to 6
- norm_gain: float32 [2048], replicated, may hold values from 0.1 to 1.9
- routes: int32 [32768, 4], P(('ep', 'tp')), may hold values from 0 to 63, all different within a row; in each aligned block of 128 rows (0 to 127, 128 to 255, ...) at most 16 rows name the same one
- route_weight: float32 [32768, 4], P(('ep', 'tp')), may hold values from 0.05 to 1
- gate_weight: bfloat16 [64, 2048, 512], P('ep'), may hold values from -2 to 2
- up_weight: bfloat16 [64, 2048, 512], P('ep'), may hold values from -2 to 2
- down_weight: bfloat16 [64, 512, 2048], P('ep'), may hold values from -0.25 to 0.25
Outputs:
- attention_out: bfloat16 [65536, 2048], P(('ep', 'tp'))
- routed_out: bfloat16 [32768, 2048], P(('ep', 'tp'))
The draws below stay inside these ranges and needn't reach their ends.
Inputs may be any that keep to these rules, and one draw needn't show every extreme that they name: `routes`: within the rows of one device (aligned blocks of 128 rows), each expert is named by at most 16 rows, and in every draw some expert by exactly 16; a row names 4 different experts.
All inputs are finite; a program needn't handle non-finite values.
Results may differ from the reference program's by a relative error of at most 0.0078.
Values may be sent and summed in bfloat16 or wider, within the bound.
A program may use at most 128 MiB of HBM per device.

```python
import math
import jax
import jax.numpy as jnp
import numpy as np
from jax import lax

D = 2048
HEADS = 16
KV_HEADS = 4
HEAD_DIM = 64
WINDOW = 128
SEQS = 1
FF = 512
TOPK = 4
TOK_M = 128
EXPERTS = 64
CAP = 16
TOKENS_A = 65536
TOKENS_M = 32768


def draw_queries(key, part):
    per_group = HEADS // KV_HEADS
    normal = jax.random.normal(jax.random.fold_in(key, 1), (TOKENS_A, KV_HEADS, per_group, HEAD_DIM), jnp.float32)
    normal = jnp.clip(normal, -6.0, 6.0)
    return normal.reshape(TOKENS_A, HEADS * HEAD_DIM).astype(jnp.bfloat16)


def draw_head_keys(key, part):
    normal = jax.random.normal(jax.random.fold_in(key, 2), (TOKENS_A, KV_HEADS, 1, HEAD_DIM), jnp.float32)
    normal = jnp.clip(normal, -6.0, 6.0)
    return normal.reshape(TOKENS_A, KV_HEADS * HEAD_DIM).astype(jnp.bfloat16)


def expert_matrix(key, salt):
    normal = jax.random.normal(jax.random.fold_in(key, salt), (EXPERTS, D, FF), jnp.float32)
    normal = jnp.clip(normal, -6.0, 6.0) * D ** (-0.5)
    return jnp.clip(normal, -2.0, 2.0).astype(jnp.bfloat16)


def draw_gate_weight(key, part):
    return expert_matrix(key, 11)


def draw_up_weight(key, part):
    return expert_matrix(key, 13)


def block_scale(stream_key, shape, pieces, low, top_value):
    factor_of, own = 1.0, jax.random.fold_in(stream_key, 6)
    for position, parts in pieces:
        draws = jnp.exp(jax.random.uniform(jax.random.fold_in(own, position), (parts,), jnp.float32, low / len(pieces), top_value / len(pieces)))
        factor_of = factor_of * jnp.repeat(draws, shape[position] // parts).reshape([-1 if axis == position else 1 for axis in range(len(shape))])
    return factor_of


def deal_out(key, own, number, rows, number_of, top, limit, lean):
    sequence = jax.random.permutation(key, number_of)
    crowded, ordinary = shares(number_of, rows * top, limit, lean, True), shares(number_of, rows * top, limit, lean, False)
    places = jnp.arange(number_of)

    def named(tallies, turn):
        used = int((tallies > 0).sum())
        fixed = max(1, used // 4)
        passed = fixed + (places - fixed + turn * (used - fixed)) % max(1, number_of - fixed)
        return jnp.zeros((number_of,), jnp.int32).at[sequence[jnp.where(places < fixed, places, passed)]].set(jnp.asarray(tallies, jnp.int32))

    tallies = jnp.where(number % 4 == 0, named(crowded, number // 4), named(ordinary, number - number // 4 - 1))
    mixed = jax.random.permutation(jax.random.fold_in(own, 3), number_of)
    giver, sink = mixed[0:number_of // 2 * 2:2], mixed[1:number_of // 2 * 2:2]
    margin = jnp.minimum(tallies[giver] - 1, limit - tallies[sink]) // 2
    margin = jnp.where((giver == sequence[0]) | (sink == sequence[0]) | (tallies[sink] == 0), 0, jnp.maximum(margin, 0))
    passed = jax.random.randint(jax.random.fold_in(own, 4), (number_of // 2,), 0, 1 << 20) % (margin + 1)
    tallies = tallies.at[giver].add(-passed).at[sink].add(passed)
    labels = jnp.searchsorted(jnp.cumsum(tallies), jnp.arange(rows * top), side="right").astype(jnp.int32)
    listing = labels.reshape(top, rows).T
    listing = listing[jax.random.permutation(jax.random.fold_in(own, 1), rows)]
    turn = jax.random.randint(jax.random.fold_in(own, 2), (rows, 1), 0, top)
    return jnp.take_along_axis(listing, (jnp.arange(top)[None, :] + turn) % top, axis=1)


def shares(number_of, total, most, skew, full):
    portions = [(1 << 20) // math.isqrt(standing ** skew) + 1 for standing in range(1, number_of + 1)]
    largest = most if full else min(most, max(-(-total // number_of), total * portions[0] // sum(portions)))
    least = 1 if total - largest >= number_of - 1 else 0
    given, rest = [largest] + [least] * (number_of - 1), total - largest - least * (number_of - 1)
    while rest > 0:
        candidates = [i for i in range(1, number_of) if given[i] < largest] or [i for i in range(1, number_of) if given[i] < most]
        mass, remaining = sum([portions[i] for i in candidates]), rest
        for i in candidates:
            addition = min(most - given[i], max(1, remaining * portions[i] // mass), rest)
            given[i] = given[i] + addition
            rest = rest - addition
    return np.array(given)


def gaussian(key, shape, spread, reach, split=(), kind=jnp.bfloat16):
    drawn = jax.random.normal(key, shape, jnp.float32) * spread
    if len(split) > 0:
        drawn = block_scale(key, shape, split, -0.22, 0.18) * drawn
    return jnp.clip(drawn, min=-reach, max=reach).astype(kind)


def setup_inputs(seed: int = 0) -> dict:
    streams_of = jax.random.split(jax.random.key(seed), 13)
    queries = draw_queries(jax.random.fold_in(streams_of[12], 71), 0)
    head_keys = draw_head_keys(jax.random.fold_in(streams_of[12], 71), 0)
    head_values = gaussian(streams_of[2], (TOKENS_A, KV_HEADS * HEAD_DIM), 1.0, 6.0, ((0, 64), (1, 4)))
    sink_logits = jnp.clip(-2.0 + 7.0 * jax.random.uniform(streams_of[3], (HEADS,), jnp.float32) ** block_scale(streams_of[3], (HEADS,), ((0, 4),), -0.2, 0.2), -2.0, 5.0)
    out_weight = gaussian(streams_of[4], (HEADS * HEAD_DIM, D), 0.25, 1.5, ((0, 4),))
    moe_input = gaussian(streams_of[5], (TOKENS_M, D), 1.0, 6.0, ((0, 256),))
    norm_gain = jnp.clip(1.0 + 0.18 * jax.random.normal(streams_of[6], (D,), jnp.float32), 0.1, 1.9)
    routes_keys = jax.random.split(jax.random.fold_in(streams_of[7], 1), TOKENS_M // TOK_M)
    routes_turns = jax.random.permutation(jax.random.fold_in(streams_of[7], 3), TOKENS_M // TOK_M)
    routes = jax.vmap(lambda own, number: deal_out(jax.random.fold_in(streams_of[7], 2), own, number, TOK_M, EXPERTS, TOPK, CAP, 1))(routes_keys, routes_turns).reshape((TOKENS_M, TOPK))
    route_weight = jnp.clip(jnp.exp(math.log(1.0) - 2.9957323 * jax.random.uniform(streams_of[8], (TOKENS_M, TOPK), jnp.float32) ** block_scale(streams_of[8], (TOKENS_M, TOPK), ((0, 256),), -0.2, 0.2)), 0.05, 1.0)
    gate_weight = draw_gate_weight(jax.random.fold_in(streams_of[12], 71), 0)
    up_weight = draw_up_weight(jax.random.fold_in(streams_of[12], 71), 0)
    down_weight = gaussian(streams_of[11], (EXPERTS, FF, D), FF ** -0.5, 0.25, ((0, 64),))
    return dict(queries=queries, head_keys=head_keys, head_values=head_values, sink_logits=sink_logits, out_weight=out_weight, moe_input=moe_input, norm_gain=norm_gain, routes=routes, route_weight=route_weight, gate_weight=gate_weight, up_weight=up_weight, down_weight=down_weight)


EPSILON = 1e-05
NEGATIVE = -1e+30

def clamped_unit(gate_pre, up_pre):
    gate_cut = jnp.minimum(gate_pre, 7.0)
    up_cut = jnp.clip(up_pre, -7.0, 7.0)
    return gate_cut * jax.nn.sigmoid(1.702 * gate_cut) * (up_cut + 1.0)

def window_attention(queries, head_keys, head_values, sink_logits, out_weight):
    total = queries.shape[0]
    per_group = HEADS // KV_HEADS
    seq_len = TOKENS_A // SEQS
    padding = jnp.zeros((WINDOW, KV_HEADS * HEAD_DIM), head_keys.dtype)
    padded_keys = jnp.concatenate([padding, head_keys], axis=0)
    padded_values = jnp.concatenate([padding, head_values], axis=0)
    sinks = sink_logits.astype(jnp.float32).reshape(KV_HEADS, per_group, 1, 1)

    def one_block(index):
        first = (index * WINDOW).astype(jnp.int32)
        block_q = lax.dynamic_slice_in_dim(queries, first, WINDOW, 0)
        block_q = block_q.reshape(WINDOW, KV_HEADS, per_group, HEAD_DIM).astype(jnp.float32)
        block_k = lax.dynamic_slice_in_dim(padded_keys, first, 2 * WINDOW, 0)
        block_k = block_k.reshape(2 * WINDOW, KV_HEADS, HEAD_DIM).astype(jnp.float32)
        block_v = lax.dynamic_slice_in_dim(padded_values, first, 2 * WINDOW, 0)
        block_v = block_v.reshape(2 * WINDOW, KV_HEADS, HEAD_DIM).astype(jnp.float32)
        scores = jnp.einsum('qkgd,skd->kgqs', block_q, block_k) * HEAD_DIM ** (-0.5)
        query_pos = first + jnp.arange(WINDOW, dtype=jnp.int32)
        key_pos = first - WINDOW + jnp.arange(2 * WINDOW, dtype=jnp.int32)
        distance = query_pos[:, None] - key_pos[None, :]
        starts = query_pos // seq_len * seq_len
        valid = (distance >= 0) & (distance < WINDOW) & (key_pos[None, :] >= starts[:, None])
        scores = jnp.where(valid[None, None], scores, NEGATIVE)
        maxima = jnp.maximum(lax.optimization_barrier(jnp.max(scores, axis=-1, keepdims=True)), sinks)
        powers = jnp.exp(scores - maxima)
        weights = powers / (lax.optimization_barrier(jnp.sum(powers, axis=-1, keepdims=True)) + jnp.exp(sinks - maxima))
        weights = weights.astype(jnp.bfloat16)
        heads = jnp.einsum('kgqs,skd->qkgd', weights.astype(jnp.float32), block_v)
        return heads.astype(jnp.bfloat16).reshape(WINDOW, HEADS * HEAD_DIM)
    heads_out = lax.map(one_block, jnp.arange(total // WINDOW, dtype=jnp.int32))
    heads_out = heads_out.reshape(total, HEADS * HEAD_DIM)
    return jnp.dot(heads_out, out_weight, preferred_element_type=jnp.float32).astype(jnp.bfloat16)

def routed_experts(moe_input, norm_gain, routes, route_weight, gate_weight, up_weight, down_weight):
    token_count = moe_input.shape[0]
    values32 = moe_input.astype(jnp.float32)
    scale = lax.rsqrt(lax.optimization_barrier(jnp.mean(values32 * values32, axis=-1, keepdims=True)) + EPSILON)
    normed = (values32 * scale * norm_gain.astype(jnp.float32)).astype(jnp.bfloat16)
    assigned = token_count * TOPK
    group_rows = 256
    flat_routes = routes.reshape(assigned).astype(jnp.int32)
    token_of = (jnp.arange(assigned, dtype=jnp.int32) // TOPK).astype(jnp.int32)
    order = jnp.argsort(flat_routes, stable=True).astype(jnp.int32)
    sorted_routes = flat_routes[order]
    counts = lax.optimization_barrier(jnp.sum((flat_routes[:, None] == jnp.arange(EXPERTS, dtype=jnp.int32)[None, :]).astype(jnp.int32), axis=0)).astype(jnp.int32)
    padded = ((counts + group_rows - 1) // group_rows * group_rows).astype(jnp.int32)
    end_pad = jnp.cumsum(padded).astype(jnp.int32)
    start_pad = (end_pad - padded).astype(jnp.int32)
    start_raw = (jnp.cumsum(counts) - counts).astype(jnp.int32)
    dest = (start_pad[sorted_routes] + jnp.arange(assigned, dtype=jnp.int32) - start_raw[sorted_routes]).astype(jnp.int32)
    group_count = -(-assigned // group_rows) + EXPERTS
    slot_total = group_count * group_rows
    row_token = jnp.zeros((slot_total,), jnp.int32).at[dest].set(token_of[order])
    row_weight = jnp.zeros((slot_total,), jnp.float32).at[dest].set(route_weight.reshape(assigned).astype(jnp.float32)[order])
    group_expert = jnp.searchsorted(end_pad, jnp.arange(group_count, dtype=jnp.int32) * group_rows, side='right')
    group_expert = jnp.minimum(group_expert, EXPERTS - 1).astype(jnp.int32)

    def add_group(total, inputs):
        expert, tokens, weights = inputs
        rows_in = normed[tokens]
        gate_pre = jnp.dot(rows_in, gate_weight[expert], preferred_element_type=jnp.float32)
        up_pre = jnp.dot(rows_in, up_weight[expert], preferred_element_type=jnp.float32)
        act = clamped_unit(gate_pre, up_pre).astype(jnp.bfloat16)
        result = jnp.dot(act, down_weight[expert], preferred_element_type=jnp.float32).astype(jnp.bfloat16)
        return (total.at[tokens].add(result.astype(jnp.float32) * weights[:, None]), None)
    initial = jnp.zeros((token_count, D), jnp.float32)
    total, _ = lax.scan(add_group, initial, (group_expert, row_token.reshape(group_count, group_rows), row_weight.reshape(group_count, group_rows)))
    return total.astype(jnp.bfloat16)

def reference(queries, head_keys, head_values, sink_logits, out_weight, moe_input, norm_gain, routes, route_weight, gate_weight, up_weight, down_weight):
    attention_out = window_attention(queries, head_keys, head_values, sink_logits, out_weight)
    routed_out = routed_experts(moe_input, norm_gain, routes, route_weight, gate_weight, up_weight, down_weight)
    return (attention_out, routed_out)
```

```python
import functools

import jax
import jax.numpy as jnp
from jax import lax
from jax.experimental import pallas as pl
from jax.experimental.pallas import tpu as pltpu
from jax.sharding import PartitionSpec as P

MESH = pl.DeviceIdType.MESH
HEAD_DIM = 64
WINDOW = 128
CAP = 16
EPSILON = 1e-05
NEGATIVE = -1e30
PIECES = 2


def clamped_unit(gate_pre, up_pre):
    gate_cut = jnp.minimum(gate_pre, 7.0)
    up_cut = jnp.clip(up_pre, -7.0, 7.0)
    return gate_cut * jax.nn.sigmoid(1.702 * gate_cut) * (up_cut + 1.0)


def bytes_wait(ref, sem):
    pltpu.make_async_copy(ref, ref, sem).wait()


def kernel(
    Z,
    L,
    X,
    S,
    x_ref,
    gain_ref,
    routes_ref,
    rweight_ref,
    q_ref,
    k_ref,
    v_ref,
    sink_ref,
    ow_hbm,
    gw_hbm,
    uw_hbm,
    dw_hbm,
    att_ref,
    out_ref,
    ag,
    tab,
    pick,
    spread,
    disp,
    recv,
    res,
    ret,
    rs_out,
    rs_in,
    gw,
    uw,
    dw,
    wall,
    kv2,
    heads,
    hall,
    ld_sem,
    tab_send,
    tab_recv,
    z_send,
    z_recv,
    y_send,
    y_recv,
    r_send,
    r_recv,
    rs_send,
    rs_recv,
    w_send,
    w_recv,
    h_send,
    h_recv,
    halo_send,
    halo_recv,
):
    T, D = x_ref.shape
    DS = D // S
    H = Z // 2
    U = (H - 1) * S + S // 2
    EP = Z * L
    rows = q_ref.shape[0]
    per_x = rows // X
    ep = lax.axis_index("ep")
    x = lax.axis_index("tp")
    z = ep // L
    me = lax.rem(ep, L)

    def dev_z(step):
        return (lax.rem(z + step + Z, Z) * L + me, x)

    def dev_l(l):
        return (z * L + l, x)

    def dev_x(step):
        return (ep, lax.rem(x + step, X))

    right_ep = (lax.rem(ep + 1, EP), x)
    left_ep = (lax.rem(ep + EP - 1, EP), x)

    loads = [
        pltpu.make_async_copy(ow_hbm, wall.at[x], ld_sem.at[0]),
        pltpu.make_async_copy(gw_hbm.at[0], gw, ld_sem.at[1]),
        pltpu.make_async_copy(uw_hbm.at[0], uw, ld_sem.at[2]),
        pltpu.make_async_copy(dw_hbm.at[0], dw, ld_sem.at[3]),
    ]
    barrier = pltpu.get_barrier_semaphore()
    met = [dev_z(r) for r in range(1, Z)]
    met += [dev_l(lax.rem(me + r, L)) for r in range(1, L)]
    met += [dev_x(r) for r in range(1, X)]
    met += [right_ep, left_ep]
    for target in met:
        pl.semaphore_signal(barrier, inc=1, device_id=target, device_id_type=MESH)
    for load in loads:
        load.start()

    values32 = x_ref[...].astype(jnp.float32)
    scale = lax.rsqrt(jnp.mean(values32 * values32, axis=-1, keepdims=True) + EPSILON)
    normed = (values32 * scale * gain_ref[...]).astype(jnp.bfloat16)
    for f in range(S):
        ag[0, f] = normed[:, f * DS : (f + 1) * DS]
    tab[0, 0:4] = routes_ref[...].astype(jnp.float32).T
    tab[0, 4:8] = rweight_ref[...].T
    kv2[0, WINDOW:] = jnp.concatenate([k_ref[...], k_ref[...]], axis=1)
    kv2[1, WINDOW:] = jnp.concatenate([v_ref[...], v_ref[...]], axis=1)

    pl.semaphore_wait(barrier, len(met))

    def tab_copy(r):
        return pltpu.make_async_remote_copy(
            src_ref=tab.at[0],
            dst_ref=tab.at[Z - r],
            send_sem=tab_send,
            recv_sem=tab_recv.at[Z - r],
            device_id=dev_z(r),
            device_id_type=MESH,
        )

    for r in range(1, Z):
        tab_copy(r).start()

    def ring_copy(direction, u):
        hop, i = u // S + 1, lax.rem(u, S)
        if direction == 0:
            f, src, dst, target = i, lax.rem(Z - hop + 1, Z), Z - hop, dev_z(1)
        else:
            f, src, dst, target = S - 1 - i, hop - 1, hop, dev_z(-1)
        return pltpu.make_async_remote_copy(
            src_ref=ag.at[src, f],
            dst_ref=ag.at[dst, f],
            send_sem=z_send.at[direction],
            recv_sem=z_recv.at[direction, u],
            device_id=target,
            device_id_type=MESH,
        )

    for u in range(min(S, U)):
        ring_copy(0, u).start()
        ring_copy(1, u).start()

    halo = pltpu.make_async_remote_copy(
        src_ref=kv2.at[:, pl.ds(rows, WINDOW)],
        dst_ref=kv2.at[:, pl.ds(0, WINDOW)],
        send_sem=halo_send,
        recv_sem=halo_recv,
        device_id=right_ep,
        device_id_type=MESH,
    )
    halo.start()

    def make_slots(o):
        table = tab[o]
        expert = (lax.broadcasted_iota(jnp.int32, (L, T), 0) + z * L).astype(jnp.float32)
        named = jnp.zeros((L, T), jnp.float32)
        weight = jnp.zeros((L, T), jnp.float32)
        for k in range(4):
            hit = table[k : k + 1, :] == expert
            named = named + jnp.where(hit, 1.0, 0.0)
            weight = weight + jnp.where(hit, table[4 + k : 5 + k, :], 0.0)
        before = (
            lax.broadcasted_iota(jnp.int32, (T, T), 0) < lax.broadcasted_iota(jnp.int32, (T, T), 1)
        ).astype(jnp.float32)
        rank = jnp.dot(named, before, preferred_element_type=jnp.float32)
        rank = jnp.where(named > 0.5, rank, -1.0)
        slot = lax.broadcasted_iota(jnp.int32, (CAP, T), 0).astype(jnp.float32)
        hits = jnp.concatenate(
            [jnp.where(rank[l : l + 1, :] == slot, 1.0, 0.0) for l in range(L)], axis=0
        )
        weights = jnp.concatenate(
            [jnp.where(rank[l : l + 1, :] == slot, weight[l : l + 1, :], 0.0) for l in range(L)],
            axis=0,
        )
        pick[o] = hits.astype(jnp.bfloat16)
        turned = weights.T
        high = turned.astype(jnp.bfloat16)
        spread[o, 0] = high
        spread[o, 1] = (turned - high.astype(jnp.float32)).astype(jnp.bfloat16)

    def dispatch(o, f):
        chosen = jnp.dot(pick[o], ag[o, f], preferred_element_type=jnp.float32)
        disp[o, f] = chosen.astype(jnp.bfloat16).reshape(L, CAP, DS)
        recv[o, f, me] = disp[o, f, me]
        for r in range(1, L):
            l = lax.rem(me + r, L)
            pltpu.make_async_remote_copy(
                src_ref=disp.at[o, f, l],
                dst_ref=recv.at[o, f, me],
                send_sem=y_send,
                recv_sem=y_recv.at[o],
                device_id=dev_l(l),
                device_id_type=MESH,
            ).start()

    def give_back(o, f):
        for r in range(1, L):
            l = lax.rem(me + r, L)
            pltpu.make_async_remote_copy(
                src_ref=res.at[o, f, l],
                dst_ref=ret.at[o, f, me],
                send_sem=r_send,
                recv_sem=r_recv.at[o, f],
                device_id=dev_l(l),
                device_id_type=MESH,
            ).start()

    def expert(o):
        bytes_wait(disp.at[o, :, pl.ds(0, L - 1)], y_recv.at[o])
        gate_pre = jnp.zeros((L * CAP, gw.shape[1]), jnp.float32)
        up_pre = jnp.zeros((L * CAP, gw.shape[1]), jnp.float32)
        for f in range(S):
            block = recv[o, f].reshape(L * CAP, DS)
            cut = slice(f * DS, (f + 1) * DS)
            gate_pre += jnp.dot(block, gw[cut, :], preferred_element_type=jnp.float32)
            up_pre += jnp.dot(block, uw[cut, :], preferred_element_type=jnp.float32)
        act = clamped_unit(gate_pre, up_pre).astype(jnp.bfloat16)
        for f in range(S):
            cut = slice(f * DS, (f + 1) * DS)
            result = jnp.dot(act, dw[:, cut], preferred_element_type=jnp.float32)
            res[o, f] = result.astype(jnp.bfloat16).reshape(L, CAP, DS)
            ret[o, f, me] = res[o, f, me]

    def combine(o, f):
        bytes_wait(res.at[o, f, pl.ds(0, L - 1)], r_recv.at[o, f])
        block = ret[o, f].reshape(L * CAP, DS)
        return jnp.dot(spread[o, 0], block, preferred_element_type=jnp.float32) + jnp.dot(
            spread[o, 1], block, preferred_element_type=jnp.float32
        )

    def job_offset(k):
        h = (k + 1) // 2
        odd = lax.rem(k, 2)
        return odd * (Z - h) + (1 - odd) * h

    make_slots(0)
    for f in range(S):
        dispatch(0, f)

    loads[0].wait()

    def weight_copy(r):
        return pltpu.make_async_remote_copy(
            src_ref=wall.at[x],
            dst_ref=wall.at[x],
            send_sem=w_send,
            recv_sem=w_recv,
            device_id=dev_x(r),
            device_id_type=MESH,
        )

    for r in range(1, X):
        weight_copy(r).start()

    blocks = rows // WINDOW

    def attend(step, carry):
        b = blocks - 1 - step

        @pl.when(b == 0)
        def _():
            halo.wait_recv()

        first = pl.multiple_of(b * WINDOW, WINDOW)
        keys = kv2[0, pl.ds(first, 2 * WINDOW), :]
        vals = kv2[1, pl.ds(first, 2 * WINDOW), :]
        qs = lax.broadcasted_iota(jnp.int32, (WINDOW, 2 * WINDOW), 0)
        ks = lax.broadcasted_iota(jnp.int32, (WINDOW, 2 * WINDOW), 1)
        lowest = jnp.where((ep == 0) & (b == 0), WINDOW, 0)
        valid = (ks > qs) & (ks <= qs + WINDOW) & (ks >= lowest)
        lower = lax.broadcasted_iota(jnp.int32, (WINDOW, 2 * HEAD_DIM), 1) < HEAD_DIM
        for pair in range(2):
            cut = slice(pair * 2 * HEAD_DIM, (pair + 1) * 2 * HEAD_DIM)
            both = q_ref[pl.ds(first, WINDOW), cut]
            halves = []
            for half in range(2):
                keep = lower if half == 0 else jnp.logical_not(lower)
                mine = jnp.where(keep, both, jnp.zeros_like(both))
                scores = lax.dot_general(
                    mine, keys, (((1,), (1,)), ((), ())), preferred_element_type=jnp.float32
                ) * HEAD_DIM ** (-0.5)
                scores = jnp.where(valid, scores, NEGATIVE)
                sink = sink_ref[2 * pair + half]
                maxima = jnp.maximum(jnp.max(scores, axis=-1, keepdims=True), sink)
                powers = jnp.exp(scores - maxima)
                total = jnp.sum(powers, axis=-1, keepdims=True) + jnp.exp(sink - maxima)
                weights = (powers / total).astype(jnp.bfloat16)
                halves.append(jnp.dot(weights, vals, preferred_element_type=jnp.float32))
            done = jnp.where(lower, halves[0], halves[1]).astype(jnp.bfloat16)
            heads[
                b * WINDOW // per_x, pl.ds(pl.multiple_of(lax.rem(b * WINDOW, per_x), WINDOW), WINDOW), cut
            ] = done
        return carry

    lax.fori_loop(0, blocks, attend, 0)
    hall[x] = heads[x]
    for r in range(1, X):
        pltpu.make_async_remote_copy(
            src_ref=heads.at[lax.rem(x + r, X)],
            dst_ref=hall.at[x],
            send_sem=h_send,
            recv_sem=h_recv,
            device_id=dev_x(r),
            device_id_type=MESH,
        ).start()

    for load in loads[1:]:
        load.wait()

    def spread_step(u, carry):
        hop, i = u // S + 1, lax.rem(u, S)
        for direction in range(2):
            ring_copy(direction, u).wait_recv()

            @pl.when(u + S < U)
            def _():
                ring_copy(direction, u + S).start()

        @pl.when(i == 0)
        def _():
            bytes_wait(tab.at[0], tab_recv.at[hop])
            make_slots(hop)

            @pl.when(hop < H)
            def _():
                bytes_wait(tab.at[0], tab_recv.at[Z - hop])
                make_slots(Z - hop)

        dispatch(Z - hop, i)
        dispatch(hop, S - 1 - i)
        half = S // 2
        k = jnp.where(u == half, 0, u // half - 2)

        @pl.when((lax.rem(u, half) == 0) & ((u == half) | (k >= 1)))
        def _():
            o = job_offset(k)
            expert(o)

            @pl.when(u == half)
            def _():
                for f in range(S):
                    give_back(0, f)

        return carry

    lax.fori_loop(0, U, spread_step, 0)

    def back_unit(u):
        hop, i = u // S + 1, lax.rem(u, S)
        give_back(Z - hop, i)
        give_back(hop, S - 1 - i)

    first_late = max(1, Z - 3)

    def late_job(k, carry):
        expert(job_offset(k))

        @pl.when(k == Z - 2)
        def _():
            back_unit(0)

        return carry

    if U <= S // 2:
        expert(0)
        for f in range(S):
            give_back(0, f)
    lax.fori_loop(first_late, Z, late_job, 0)

    ahead = 3
    for j in range(ahead):
        if U - 1 - j >= 1:
            back_unit(U - 1 - j)

    def rs_copy(direction, u):
        return pltpu.make_async_remote_copy(
            src_ref=rs_out.at[direction, u],
            dst_ref=rs_in.at[direction, u],
            send_sem=rs_send.at[direction],
            recv_sem=rs_recv.at[direction, u],
            device_id=dev_z(1 if direction == 0 else -1),
            device_id_type=MESH,
        )

    for direction in range(2):
        for u in range(U, U + S):
            rs_in[direction, u] = jnp.zeros((T, DS), jnp.bfloat16)

    def gather_step(v, carry):
        u = U - 1 - v
        hop, i = u // S + 1, lax.rem(u, S)

        @pl.when(u - ahead >= 1)
        def _():
            back_unit(u - ahead)

        for direction in range(2):
            o, f = (hop, S - 1 - i) if direction == 0 else (Z - hop, i)
            value = combine(o, f)

            @pl.when(u + S < U)
            def _():
                rs_copy(direction, u + S).wait_recv()

            value = value + rs_in[direction, u + S].astype(jnp.float32)
            rs_out[direction, u] = value.astype(jnp.bfloat16)
            rs_copy(direction, u).start()

        @pl.when(v == 1)
        def _():
            bytes_wait(wall.at[pl.ds(0, X - 1)], w_recv)
            bytes_wait(hall.at[pl.ds(0, X - 1)], h_recv)
            wide = att_ref.shape[1] // 4
            for n in range(4):
                cut = slice(n * wide, (n + 1) * wide)
                total = jnp.dot(hall[0], wall[0, :, cut], preferred_element_type=jnp.float32)
                for s in range(1, X):
                    total += jnp.dot(hall[s], wall[s, :, cut], preferred_element_type=jnp.float32)
                att_ref[:, cut] = total.astype(jnp.bfloat16)

        return carry

    lax.fori_loop(0, U, gather_step, 0)

    for f in range(S):
        value = combine(0, f)
        rs_copy(0, S - 1 - f).wait_recv()
        rs_copy(1, f).wait_recv()
        value = value + rs_in[0, S - 1 - f].astype(jnp.float32) + rs_in[1, f].astype(jnp.float32)
        out_ref[:, f * DS : (f + 1) * DS] = value.astype(jnp.bfloat16)

    bytes_wait(tab.at[pl.ds(0, Z - 1)], tab_send)
    for direction in range(2):
        bytes_wait(rs_in.at[direction, pl.ds(0, U)], z_send.at[direction])
        bytes_wait(rs_in.at[direction, pl.ds(0, U)], rs_send.at[direction])
    bytes_wait(disp.at[:, :, pl.ds(0, L - 1)], y_send)
    bytes_wait(res.at[:, :, pl.ds(0, L - 1)], r_send)
    bytes_wait(wall.at[pl.ds(0, X - 1)], w_send)
    bytes_wait(heads.at[pl.ds(0, X - 1)], h_send)
    halo.wait_send()


def on_device(
    Z,
    L,
    X,
    queries,
    head_keys,
    head_values,
    sink_logits,
    out_weight,
    moe_input,
    norm_gain,
    routes,
    route_weight,
    gate_weight,
    up_weight,
    down_weight,
):
    S = PIECES
    T, D = moe_input.shape
    DS = D // S
    FF = gate_weight.shape[2]
    rows, cols = queries.shape
    H = Z // 2
    U = (H - 1) * S + S // 2
    slots = L * CAP
    bf16, f32 = jnp.bfloat16, jnp.float32
    vmem = pl.BlockSpec(memory_space=pltpu.VMEM)
    hbm = pl.BlockSpec(memory_space=pl.ANY)
    dma = pltpu.SemaphoreType.DMA
    attention_out, routed_out = pl.pallas_call(
        functools.partial(kernel, Z, L, X, S),
        out_shape=(
            jax.ShapeDtypeStruct((rows // X, D), bf16),
            jax.ShapeDtypeStruct((T, D), bf16),
        ),
        in_specs=[vmem] * 7 + [pl.BlockSpec(memory_space=pltpu.SMEM)] + [hbm] * 4,
        out_specs=(vmem, vmem),
        scratch_shapes=[
            pltpu.VMEM((Z, S, T, DS), bf16),
            pltpu.VMEM((Z, 8, T), f32),
            pltpu.VMEM((Z, slots, T), bf16),
            pltpu.VMEM((Z, 2, T, slots), bf16),
            pltpu.VMEM((Z, S, L, CAP, DS), bf16),
            pltpu.VMEM((Z, S, L, CAP, DS), bf16),
            pltpu.VMEM((Z, S, L, CAP, DS), bf16),
            pltpu.VMEM((Z, S, L, CAP, DS), bf16),
            pltpu.VMEM((2, U, T, DS), bf16),
            pltpu.VMEM((2, U + S, T, DS), bf16),
            pltpu.VMEM((D, FF), bf16),
            pltpu.VMEM((D, FF), bf16),
            pltpu.VMEM((FF, D), bf16),
            pltpu.VMEM((X, cols, D), bf16),
            pltpu.VMEM((2, rows + WINDOW, 2 * HEAD_DIM), bf16),
            pltpu.VMEM((X, rows // X, cols), bf16),
            pltpu.VMEM((X, rows // X, cols), bf16),
            dma((4,)),
            dma,
            dma((Z,)),
            dma((2,)),
            dma((2, U)),
            dma,
            dma((Z,)),
            dma,
            dma((Z, S)),
            dma((2,)),
            dma((2, U)),
            dma,
            dma,
            dma,
            dma,
            dma,
            dma,
        ],
        compiler_params=pltpu.CompilerParams(
            collective_id=0, has_side_effects=True, vmem_limit_bytes=60 * 1024 * 1024
        ),
    )(
        moe_input,
        norm_gain.reshape(1, D),
        routes,
        route_weight,
        queries,
        head_keys,
        head_values,
        sink_logits,
        out_weight,
        gate_weight,
        up_weight,
        down_weight,
    )
    return (attention_out, routed_out)


def solution(mesh, layer=8):
    X = mesh.shape["tp"]
    Z = mesh.shape["ep"] // layer
    placed = (
        P("ep", "tp"),
        P("ep", "tp"),
        P("ep", "tp"),
        P("tp"),
        P("tp", None),
        P(("ep", "tp"), None),
        P(),
        P(("ep", "tp"), None),
        P(("ep", "tp"), None),
        P("ep", None, None),
        P("ep", None, None),
        P("ep", None, None),
    )
    return jax.shard_map(
        functools.partial(on_device, Z, layer, X),
        mesh=mesh,
        in_specs=placed,
        out_specs=(P(("ep", "tp"), None), P(("ep", "tp"), None)),
        check_vma=False,
    )
```

```python
import functools

import jax
import jax.numpy as jnp
from jax import lax
from jax.experimental import pallas as pl
from jax.experimental.pallas import tpu as pltpu
from jax.sharding import PartitionSpec as P

MESH = pl.DeviceIdType.MESH
HEAD_DIM = 64
WINDOW = 128
CAP = 16
EPSILON = 1e-05
NEGATIVE = -1e30
PIECES = 4
AHEAD = 4
EARLY = 3
FILL = 1


def clamped_unit(gate_pre, up_pre):
    gate_cut = jnp.minimum(gate_pre, 7.0)
    up_cut = jnp.clip(up_pre, -7.0, 7.0)
    return gate_cut * jax.nn.sigmoid(1.702 * gate_cut) * (up_cut + 1.0)


def bytes_wait(ref, sem):
    if 0 in ref.shape:
        return
    pltpu.make_async_copy(ref, ref, sem).wait()


def kernel(
    Z,
    L,
    X,
    S,
    x_ref,
    gain_ref,
    routes_ref,
    rweight_ref,
    q_ref,
    k_ref,
    v_ref,
    sink_ref,
    ow_hbm,
    gw_hbm,
    uw_hbm,
    dw_hbm,
    att_ref,
    out_ref,
    ag,
    tab,
    pick,
    spread,
    disp,
    recv,
    res,
    ret,
    rs_out,
    rs_in,
    gw,
    uw,
    dw,
    wall,
    kv2,
    heads,
    hall,
    ld_sem,
    tab_send,
    tab_recv,
    z_send,
    z_recv,
    y_send,
    y_recv,
    r_send,
    r_recv,
    rs_send,
    rs_recv,
    w_send,
    w_recv,
    h_send,
    h_recv,
    halo_send,
    halo_recv,
):
    T, D = x_ref.shape
    DS = D // S
    H = Z // 2
    U = (H - 1) * S + S // 2
    EP = Z * L
    rows = q_ref.shape[0]
    per_x = rows // X
    ep = lax.axis_index("ep")
    x = lax.axis_index("tp")
    z = ep // L
    me = lax.rem(ep, L)

    def dev_z(step):
        return (lax.rem(z + step + Z, Z) * L + me, x)

    def dev_l(l):
        return (z * L + l, x)

    def dev_x(step):
        return (ep, lax.rem(x + step, X))

    right_ep = (lax.rem(ep + 1, EP), x)
    left_ep = (lax.rem(ep + EP - 1, EP), x)

    loads = [
        pltpu.make_async_copy(ow_hbm, wall.at[x], ld_sem.at[0]),
        pltpu.make_async_copy(gw_hbm.at[0], gw, ld_sem.at[1]),
        pltpu.make_async_copy(uw_hbm.at[0], uw, ld_sem.at[2]),
        pltpu.make_async_copy(dw_hbm.at[0], dw, ld_sem.at[3]),
    ]
    barrier = pltpu.get_barrier_semaphore()
    met = [dev_z(1), dev_z(-1)]
    met += [dev_l(lax.rem(me + r, L)) for r in range(1, L)]
    met += [dev_x(r) for r in range(1, X)]
    met += [right_ep, left_ep]
    for target in met:
        pl.semaphore_signal(barrier, inc=1, device_id=target, device_id_type=MESH)
    for load in loads:
        load.start()

    values32 = x_ref[...].astype(jnp.float32)
    scale = lax.rsqrt(jnp.mean(values32 * values32, axis=-1, keepdims=True) + EPSILON)
    normed = (values32 * scale * gain_ref[...]).astype(jnp.bfloat16)
    for f in range(S):
        ag[0, f] = normed[:, f * DS : (f + 1) * DS]
    tab[0, 0:4] = routes_ref[...].astype(jnp.float32)
    tab[0, 4:8] = rweight_ref[...]
    for half in range(2):
        cut = slice(half * HEAD_DIM, (half + 1) * HEAD_DIM)
        kv2[0, cut, WINDOW:] = k_ref[...]
        kv2[1, cut, WINDOW:] = v_ref[...]

    pl.semaphore_wait(barrier, len(met))

    halo = pltpu.make_async_remote_copy(
        src_ref=kv2.at[:, :, pl.ds(rows, WINDOW)],
        dst_ref=kv2.at[:, :, pl.ds(0, WINDOW)],
        send_sem=halo_send,
        recv_sem=halo_recv,
        device_id=right_ep,
        device_id_type=MESH,
    )
    halo.start()

    def tab_copy(direction, hop):
        if direction == 0:
            src, dst, target = lax.rem(Z - hop + 1, Z), Z - hop, dev_z(1)
        else:
            src, dst, target = hop - 1, hop, dev_z(-1)
        return pltpu.make_async_remote_copy(
            src_ref=tab.at[src],
            dst_ref=tab.at[dst],
            send_sem=tab_send,
            recv_sem=tab_recv.at[dst],
            device_id=target,
            device_id_type=MESH,
        )

    tab_copy(0, 1).start()
    if H > 1:
        tab_copy(1, 1).start()

    def ring_copy(direction, u):
        hop, i = u // S + 1, lax.rem(u, S)
        if direction == 0:
            f, src, dst, target = i, lax.rem(Z - hop + 1, Z), Z - hop, dev_z(1)
        else:
            f, src, dst, target = S - 1 - i, hop - 1, hop, dev_z(-1)
        return pltpu.make_async_remote_copy(
            src_ref=ag.at[src, f],
            dst_ref=ag.at[dst, f],
            send_sem=z_send.at[direction],
            recv_sem=z_recv.at[direction, u],
            device_id=target,
            device_id_type=MESH,
        )

    for u in range(min(S, U)):
        ring_copy(0, u).start()
        ring_copy(1, u).start()

    def make_slots(o):
        table = tab[o]
        expert = (lax.broadcasted_iota(jnp.int32, (L, T), 0) + z * L).astype(jnp.float32)
        named = jnp.zeros((L, T), jnp.float32)
        weight = jnp.zeros((L, T), jnp.float32)
        for k in range(4):
            hit = table[k : k + 1, :] == expert
            named = named + jnp.where(hit, 1.0, 0.0)
            weight = weight + jnp.where(hit, table[4 + k : 5 + k, :], 0.0)
        before = (
            lax.broadcasted_iota(jnp.int32, (T, T), 0) < lax.broadcasted_iota(jnp.int32, (T, T), 1)
        ).astype(jnp.float32)
        rank = jnp.dot(named, before, preferred_element_type=jnp.float32)
        rank = jnp.where(named > 0.5, rank, -1.0)
        slot = lax.broadcasted_iota(jnp.int32, (CAP, T), 0).astype(jnp.float32)
        hits = jnp.concatenate(
            [jnp.where(rank[l : l + 1, :] == slot, 1.0, 0.0) for l in range(L)], axis=0
        )
        weights = jnp.concatenate(
            [jnp.where(rank[l : l + 1, :] == slot, weight[l : l + 1, :], 0.0) for l in range(L)],
            axis=0,
        )
        pick[o] = hits.astype(jnp.bfloat16)
        turned = weights.T
        high = turned.astype(jnp.bfloat16)
        spread[o, 0] = high
        spread[o, 1] = (turned - high.astype(jnp.float32)).astype(jnp.bfloat16)

    def dispatch(o, f):
        chosen = jnp.dot(pick[o], ag[o, f], preferred_element_type=jnp.float32)
        disp[o, f] = chosen.astype(jnp.bfloat16).reshape(L, CAP, DS)
        recv[o, f, me] = disp[o, f, me]
        for r in range(1, L):
            l = lax.rem(me + r, L)
            pltpu.make_async_remote_copy(
                src_ref=disp.at[o, f, l],
                dst_ref=recv.at[o, f, me],
                send_sem=y_send,
                recv_sem=y_recv.at[o],
                device_id=dev_l(l),
                device_id_type=MESH,
            ).start()

    def give_back(o, f):
        for r in range(1, L):
            l = lax.rem(me + r, L)
            pltpu.make_async_remote_copy(
                src_ref=res.at[o, f, l],
                dst_ref=ret.at[o, f, me],
                send_sem=r_send,
                recv_sem=r_recv.at[o, f],
                device_id=dev_l(l),
                device_id_type=MESH,
            ).start()

    def expert(o):
        bytes_wait(disp.at[o, :, pl.ds(0, L - 1)], y_recv.at[o])
        gate_pre = jnp.zeros((L * CAP, gw.shape[1]), jnp.float32)
        up_pre = jnp.zeros((L * CAP, gw.shape[1]), jnp.float32)
        for f in range(S):
            block = recv[o, f].reshape(L * CAP, DS)
            cut = slice(f * DS, (f + 1) * DS)
            gate_pre += jnp.dot(block, gw[cut, :], preferred_element_type=jnp.float32)
            up_pre += jnp.dot(block, uw[cut, :], preferred_element_type=jnp.float32)
        act = clamped_unit(gate_pre, up_pre).astype(jnp.bfloat16)
        for f in range(S):
            cut = slice(f * DS, (f + 1) * DS)
            result = jnp.dot(act, dw[:, cut], preferred_element_type=jnp.float32)
            res[o, f] = result.astype(jnp.bfloat16).reshape(L, CAP, DS)
            ret[o, f, me] = res[o, f, me]

    def combine(o, f):
        bytes_wait(res.at[o, f, pl.ds(0, L - 1)], r_recv.at[o, f])
        block = ret[o, f].reshape(L * CAP, DS)
        return jnp.dot(spread[o, 0], block, preferred_element_type=jnp.float32) + jnp.dot(
            spread[o, 1], block, preferred_element_type=jnp.float32
        )

    def job_offset(k):
        h = (k + 1) // 2
        odd = lax.rem(k, 2)
        return odd * (Z - h) + (1 - odd) * h

    make_slots(0)
    for f in range(EARLY):
        dispatch(0, f)

    loads[0].wait()

    def weight_copy(r):
        return pltpu.make_async_remote_copy(
            src_ref=wall.at[x],
            dst_ref=wall.at[x],
            send_sem=w_send,
            recv_sem=w_recv,
            device_id=dev_x(r),
            device_id_type=MESH,
        )

    for r in range(1, X):
        weight_copy(r).start()

    blocks = rows // WINDOW

    def attend(step, carry):
        b = blocks - 1 - step
        first = pl.multiple_of(b * WINDOW, WINDOW)
        keys = kv2[0, :, pl.ds(first, 2 * WINDOW)]
        vals = kv2[1, :, pl.ds(first, 2 * WINDOW)]
        qs = lax.broadcasted_iota(jnp.int32, (WINDOW, 2 * WINDOW), 0)
        ks = lax.broadcasted_iota(jnp.int32, (WINDOW, 2 * WINDOW), 1)
        lowest = jnp.where((ep == 0) & (b == 0), WINDOW, 0)
        valid = (ks > qs) & (ks <= qs + WINDOW) & (ks >= lowest)
        lower = lax.broadcasted_iota(jnp.int32, (WINDOW, 2 * HEAD_DIM), 1) < HEAD_DIM
        for pair in range(2):
            cut = slice(pair * 2 * HEAD_DIM, (pair + 1) * 2 * HEAD_DIM)
            both = q_ref[pl.ds(first, WINDOW), cut]
            halves = []
            for half in range(2):
                keep = lower if half == 0 else jnp.logical_not(lower)
                mine = jnp.where(keep, both, jnp.zeros_like(both))
                scores = jnp.dot(mine, keys, preferred_element_type=jnp.float32) * HEAD_DIM ** (-0.5)
                scores = jnp.where(valid, scores, NEGATIVE)
                sink = sink_ref[2 * pair + half]
                maxima = jnp.maximum(jnp.max(scores, axis=-1, keepdims=True), sink)
                powers = jnp.exp(scores - maxima)
                total = jnp.sum(powers, axis=-1, keepdims=True) + jnp.exp(sink - maxima)
                weights = (powers / total).astype(jnp.bfloat16)
                halves.append(
                    lax.dot_general(
                        weights, vals, (((1,), (1,)), ((), ())), preferred_element_type=jnp.float32
                    )
                )
            done = jnp.where(lower, halves[0], halves[1]).astype(jnp.bfloat16)
            heads[
                b * WINDOW // per_x, pl.ds(pl.multiple_of(lax.rem(b * WINDOW, per_x), WINDOW), WINDOW), cut
            ] = done
        return carry

    lax.fori_loop(0, blocks - 1, attend, 0)

    def finish_heads():
        halo.wait_recv()
        attend(blocks - 1, 0)
        hall[x] = heads[x]
        for r in range(1, X):
            send_heads(r)

    def send_heads(r):
        pltpu.make_async_remote_copy(
            src_ref=heads.at[lax.rem(x + r, X)],
            dst_ref=hall.at[x],
            send_sem=h_send,
            recv_sem=h_recv,
            device_id=dev_x(r),
            device_id_type=MESH,
        ).start()

    for load in loads[1:]:
        load.wait()

    def spread_step(u, carry):
        hop, i = u // S + 1, lax.rem(u, S)
        for direction in range(2):
            ring_copy(direction, u).wait_recv()

            @pl.when(u + S < U)
            def _():
                ring_copy(direction, u + S).start()

        @pl.when(i == 0)
        def _():
            bytes_wait(tab.at[0], tab_recv.at[Z - hop])

            @pl.when(hop < H)
            def _():
                tab_copy(0, hop + 1).start()
                bytes_wait(tab.at[0], tab_recv.at[hop])
                make_slots(hop)

            @pl.when(hop < H - 1)
            def _():
                tab_copy(1, hop + 1).start()

            make_slots(Z - hop)

        dispatch(Z - hop, i)
        dispatch(hop, S - 1 - i)
        half = S // 2
        k = u // half - 2

        @pl.when((lax.rem(u, half) == 0) & (k >= 1))
        def _():
            expert(job_offset(k))

        @pl.when(u == S - 1)
        def _():
            finish_heads()

        return carry

    lax.fori_loop(0, U, spread_step, 0)

    def back_unit(u):
        hop, i = u // S + 1, lax.rem(u, S)
        give_back(Z - hop, i)
        give_back(hop, S - 1 - i)

    first_late = max(1, Z - 3)

    def late_job(k, carry):
        expert(job_offset(k))
        return carry

    for f in range(EARLY, S):
        dispatch(0, f)
    for u in range(FILL):
        back_unit(u)
    lax.fori_loop(first_late, Z, late_job, 0)

    ahead = min(AHEAD, U)
    for j in range(ahead):
        back_unit(U - 1 - j)

    def rs_copy(direction, u):
        return pltpu.make_async_remote_copy(
            src_ref=rs_out.at[direction, u],
            dst_ref=rs_in.at[direction, u],
            send_sem=rs_send.at[direction],
            recv_sem=rs_recv.at[direction, u],
            device_id=dev_z(1 if direction == 0 else -1),
            device_id_type=MESH,
        )

    for direction in range(2):
        for u in range(U, U + S):
            rs_in[direction, u] = jnp.zeros((T, DS), jnp.bfloat16)

    def gather_step(v, carry):
        u = U - 1 - v
        hop, i = u // S + 1, lax.rem(u, S)

        @pl.when(u - ahead >= FILL)
        def _():
            back_unit(u - ahead)

        @pl.when(v == 1)
        def _():
            expert(0)

        @pl.when(u == ahead + FILL - 1)
        def _():
            for f in range(S):
                give_back(0, f)

        for direction in range(2):
            o, f = (hop, S - 1 - i) if direction == 0 else (Z - hop, i)
            value = combine(o, f)

            @pl.when(u + S < U)
            def _():
                rs_copy(direction, u + S).wait_recv()

            value = value + rs_in[direction, u + S].astype(jnp.float32)
            rs_out[direction, u] = value.astype(jnp.bfloat16)
            rs_copy(direction, u).start()

        first = U // 2
        wide = att_ref.shape[1] // 4

        @pl.when(v == first)
        def _():
            bytes_wait(wall.at[pl.ds(0, X - 1)], w_recv)
            bytes_wait(hall.at[pl.ds(0, X - 1)], h_recv)

        @pl.when((v >= first) & (v < first + 4))
        def _():
            cut = pl.ds(pl.multiple_of((v - first) * wide, wide), wide)
            total = jnp.dot(hall[0], wall[0, :, cut], preferred_element_type=jnp.float32)
            for s in range(1, X):
                total += jnp.dot(hall[s], wall[s, :, cut], preferred_element_type=jnp.float32)
            att_ref[:, cut] = total.astype(jnp.bfloat16)

        return carry

    lax.fori_loop(0, U, gather_step, 0)

    for f in range(S):
        value = combine(0, f)
        rs_copy(0, S - 1 - f).wait_recv()
        rs_copy(1, f).wait_recv()
        value = value + rs_in[0, S - 1 - f].astype(jnp.float32) + rs_in[1, f].astype(jnp.float32)
        out_ref[:, f * DS : (f + 1) * DS] = value.astype(jnp.bfloat16)

    bytes_wait(tab.at[pl.ds(0, Z - 1)], tab_send)
    for direction in range(2):
        bytes_wait(rs_in.at[direction, pl.ds(0, U)], z_send.at[direction])
        bytes_wait(rs_in.at[direction, pl.ds(0, U)], rs_send.at[direction])
    bytes_wait(disp.at[:, :, pl.ds(0, L - 1)], y_send)
    bytes_wait(res.at[:, :, pl.ds(0, L - 1)], r_send)
    bytes_wait(wall.at[pl.ds(0, X - 1)], w_send)
    bytes_wait(heads.at[pl.ds(0, X - 1)], h_send)
    halo.wait_send()


def on_device(
    Z,
    L,
    X,
    queries,
    head_keys,
    head_values,
    sink_logits,
    out_weight,
    moe_input,
    norm_gain,
    routes,
    route_weight,
    gate_weight,
    up_weight,
    down_weight,
):
    S = PIECES
    T, D = moe_input.shape
    DS = D // S
    FF = gate_weight.shape[2]
    rows, cols = queries.shape
    H = Z // 2
    U = (H - 1) * S + S // 2
    slots = L * CAP
    bf16, f32 = jnp.bfloat16, jnp.float32
    vmem = pl.BlockSpec(memory_space=pltpu.VMEM)
    hbm = pl.BlockSpec(memory_space=pl.ANY)
    dma = pltpu.SemaphoreType.DMA
    attention_out, routed_out = pl.pallas_call(
        functools.partial(kernel, Z, L, X, S),
        out_shape=(
            jax.ShapeDtypeStruct((rows // X, D), bf16),
            jax.ShapeDtypeStruct((T, D), bf16),
        ),
        in_specs=[vmem] * 7 + [pl.BlockSpec(memory_space=pltpu.SMEM)] + [hbm] * 4,
        out_specs=(vmem, vmem),
        scratch_shapes=[
            pltpu.VMEM((Z, S, T, DS), bf16),
            pltpu.VMEM((Z, 8, T), f32),
            pltpu.VMEM((Z, slots, T), bf16),
            pltpu.VMEM((Z, 2, T, slots), bf16),
            pltpu.VMEM((Z, S, L, CAP, DS), bf16),
            pltpu.VMEM((Z, S, L, CAP, DS), bf16),
            pltpu.VMEM((Z, S, L, CAP, DS), bf16),
            pltpu.VMEM((Z, S, L, CAP, DS), bf16),
            pltpu.VMEM((2, U, T, DS), bf16),
            pltpu.VMEM((2, U + S, T, DS), bf16),
            pltpu.VMEM((D, FF), bf16),
            pltpu.VMEM((D, FF), bf16),
            pltpu.VMEM((FF, D), bf16),
            pltpu.VMEM((X, cols, D), bf16),
            pltpu.VMEM((2, 2 * HEAD_DIM, rows + WINDOW), bf16),
            pltpu.VMEM((X, rows // X, cols), bf16),
            pltpu.VMEM((X, rows // X, cols), bf16),
            dma((4,)),
            dma,
            dma((Z,)),
            dma((2,)),
            dma((2, U)),
            dma,
            dma((Z,)),
            dma,
            dma((Z, S)),
            dma((2,)),
            dma((2, U)),
            dma,
            dma,
            dma,
            dma,
            dma,
            dma,
        ],
        compiler_params=pltpu.CompilerParams(
            collective_id=0, has_side_effects=True, vmem_limit_bytes=60 * 1024 * 1024
        ),
    )(
        moe_input,
        norm_gain.reshape(1, D),
        routes.T,
        route_weight.T,
        queries,
        head_keys.T,
        head_values.T,
        sink_logits,
        out_weight,
        gate_weight,
        up_weight,
        down_weight,
    )
    return (attention_out, routed_out)


def solution(mesh, layer=8):
    X = mesh.shape["tp"]
    Z = mesh.shape["ep"] // layer
    placed = (
        P("ep", "tp"),
        P("ep", "tp"),
        P("ep", "tp"),
        P("tp"),
        P("tp", None),
        P(("ep", "tp"), None),
        P(),
        P(("ep", "tp"), None),
        P(("ep", "tp"), None),
        P("ep", None, None),
        P("ep", None, None),
        P("ep", None, None),
    )
    return jax.shard_map(
        functools.partial(on_device, Z, layer, X),
        mesh=mesh,
        in_specs=placed,
        out_specs=(P(("ep", "tp"), None), P(("ep", "tp"), None)),
        check_vma=False,
    )
```

```python
import functools

import jax
import jax.numpy as jnp
from jax import lax
from jax.experimental import pallas as pl
from jax.experimental.pallas import tpu as pltpu
from jax.sharding import PartitionSpec as P

MESH = pl.DeviceIdType.MESH
HEAD_DIM = 64
WINDOW = 128
CAP = 16
EPSILON = 1e-05
NEGATIVE = -1e30
PIECES = 8
AHEAD = 6
LATE = 2


def clamped_unit(gate_pre, up_pre):
    gate_cut = jnp.minimum(gate_pre, 7.0)
    up_cut = jnp.clip(up_pre, -7.0, 7.0)
    return gate_cut * jax.nn.sigmoid(1.702 * gate_cut) * (up_cut + 1.0)


def bytes_wait(ref, sem):
    if 0 in ref.shape:
        return
    pltpu.make_async_copy(ref, ref, sem).wait()


def kernel(
    Z,
    L,
    X,
    S,
    x_hbm,
    gain_hbm,
    routes_hbm,
    rweight_hbm,
    q_hbm,
    k_hbm,
    v_hbm,
    sink_hbm,
    ow_hbm,
    gw_hbm,
    uw_hbm,
    dw_hbm,
    att_ref,
    out_ref,
    x_ref,
    gain_ref,
    routes_ref,
    rweight_ref,
    q_ref,
    k_ref,
    v_ref,
    sink_ref,
    ag,
    tab,
    pick,
    spread,
    disp,
    recv,
    res,
    ret,
    rs_out,
    rs_in,
    gw,
    uw,
    dw,
    wall,
    kv2,
    heads,
    hall,
    ld_sem,
    tab_send,
    tab_recv,
    z_send,
    z_recv,
    y_send,
    y_recv,
    r_send,
    r_recv,
    rs_send,
    rs_recv,
    w_send,
    w_recv,
    h_send,
    h_recv,
    halo_send,
    halo_recv,
):
    T, D = x_ref.shape
    DS = D // S
    H = Z // 2
    U = (H - 1) * S + S // 2
    EP = Z * L
    rows = q_ref.shape[0]
    per_x = rows // X
    ep = lax.axis_index("ep")
    x = lax.axis_index("tp")
    z = ep // L
    me = lax.rem(ep, L)

    def dev_z(step):
        return (lax.rem(z + step + Z, Z) * L + me, x)

    def dev_l(l):
        return (z * L + l, x)

    def dev_x(step):
        return (ep, lax.rem(x + step, X))

    right_ep = (lax.rem(ep + 1, EP), x)
    left_ep = (lax.rem(ep + EP - 1, EP), x)

    pairs = [
        (x_hbm, x_ref),
        (gain_hbm, gain_ref),
        (routes_hbm, routes_ref),
        (rweight_hbm, rweight_ref),
        (k_hbm, k_ref),
        (v_hbm, v_ref),
        (ow_hbm, wall.at[x]),
        (q_hbm, q_ref),
        (sink_hbm, sink_ref),
        (gw_hbm.at[0], gw),
        (uw_hbm.at[0], uw),
        (dw_hbm.at[0], dw),
    ]
    loads = [pltpu.make_async_copy(a, b, ld_sem.at[n]) for n, (a, b) in enumerate(pairs)]
    barrier = pltpu.get_barrier_semaphore()
    met = [dev_z(1), dev_z(-1)]
    met += [dev_l(lax.rem(me + r, L)) for r in range(1, L)]
    met += [dev_x(r) for r in range(1, X)]
    met += [right_ep, left_ep]
    for target in met:
        pl.semaphore_signal(barrier, inc=1, device_id=target, device_id_type=MESH)
    for load in loads[:6]:
        load.start()

    for load in loads[:2]:
        load.wait()
    values32 = x_ref[...].astype(jnp.float32)
    scale = lax.rsqrt(jnp.mean(values32 * values32, axis=-1, keepdims=True) + EPSILON)
    normed = (values32 * scale * gain_ref[...]).astype(jnp.bfloat16)
    for f in range(S):
        ag[0, f] = normed[:, f * DS : (f + 1) * DS]
    for load in loads[2:6]:
        load.wait()
    for load in loads[6:]:
        load.start()
    tab[0, 0:4] = routes_ref[...].astype(jnp.float32)
    tab[0, 4:8] = rweight_ref[...]
    for half in range(2):
        cut = slice(half * HEAD_DIM, (half + 1) * HEAD_DIM)
        kv2[0, cut, WINDOW:] = k_ref[...]
        kv2[1, cut, WINDOW:] = v_ref[...]

    pl.semaphore_wait(barrier, len(met))

    halo = pltpu.make_async_remote_copy(
        src_ref=kv2.at[:, :, pl.ds(rows, WINDOW)],
        dst_ref=kv2.at[:, :, pl.ds(0, WINDOW)],
        send_sem=halo_send,
        recv_sem=halo_recv,
        device_id=right_ep,
        device_id_type=MESH,
    )
    halo.start()

    def tab_copy(direction, hop):
        if direction == 0:
            src, dst, target = lax.rem(Z - hop + 1, Z), Z - hop, dev_z(1)
        else:
            src, dst, target = hop - 1, hop, dev_z(-1)
        return pltpu.make_async_remote_copy(
            src_ref=tab.at[src],
            dst_ref=tab.at[dst],
            send_sem=tab_send,
            recv_sem=tab_recv.at[dst],
            device_id=target,
            device_id_type=MESH,
        )

    tab_copy(0, 1).start()
    if H > 1:
        tab_copy(1, 1).start()

    def ring_copy(direction, u):
        hop, i = u // S + 1, lax.rem(u, S)
        if direction == 0:
            f, src, dst, target = i, lax.rem(Z - hop + 1, Z), Z - hop, dev_z(1)
        else:
            f, src, dst, target = S - 1 - i, hop - 1, hop, dev_z(-1)
        return pltpu.make_async_remote_copy(
            src_ref=ag.at[src, f],
            dst_ref=ag.at[dst, f],
            send_sem=z_send.at[direction],
            recv_sem=z_recv.at[direction, u],
            device_id=target,
            device_id_type=MESH,
        )

    for u in range(min(S, U)):
        ring_copy(0, u).start()
        ring_copy(1, u).start()

    def make_slots(o):
        table = tab[o]
        expert = (lax.broadcasted_iota(jnp.int32, (L, T), 0) + z * L).astype(jnp.float32)
        named = jnp.zeros((L, T), jnp.float32)
        weight = jnp.zeros((L, T), jnp.float32)
        for k in range(4):
            hit = table[k : k + 1, :] == expert
            named = named + jnp.where(hit, 1.0, 0.0)
            weight = weight + jnp.where(hit, table[4 + k : 5 + k, :], 0.0)
        before = (
            lax.broadcasted_iota(jnp.int32, (T, T), 0) < lax.broadcasted_iota(jnp.int32, (T, T), 1)
        ).astype(jnp.float32)
        rank = jnp.dot(named, before, preferred_element_type=jnp.float32)
        rank = jnp.where(named > 0.5, rank, -1.0)
        slot = lax.broadcasted_iota(jnp.int32, (CAP, T), 0).astype(jnp.float32)
        hits = jnp.concatenate(
            [jnp.where(rank[l : l + 1, :] == slot, 1.0, 0.0) for l in range(L)], axis=0
        )
        weights = jnp.concatenate(
            [jnp.where(rank[l : l + 1, :] == slot, weight[l : l + 1, :], 0.0) for l in range(L)],
            axis=0,
        )
        pick[o] = hits.astype(jnp.bfloat16)
        turned = weights.T
        high = turned.astype(jnp.bfloat16)
        spread[o, 0] = high
        spread[o, 1] = (turned - high.astype(jnp.float32)).astype(jnp.bfloat16)

    def dispatch(o, f):
        chosen = jnp.dot(pick[o], ag[o, f], preferred_element_type=jnp.float32)
        disp[o, f] = chosen.astype(jnp.bfloat16).reshape(L, CAP, DS)
        recv[o, f, me] = disp[o, f, me]
        for r in range(1, L):
            l = lax.rem(me + r, L)
            pltpu.make_async_remote_copy(
                src_ref=disp.at[o, f, l],
                dst_ref=recv.at[o, f, me],
                send_sem=y_send,
                recv_sem=y_recv.at[o],
                device_id=dev_l(l),
                device_id_type=MESH,
            ).start()

    def give_back(o, f):
        for r in range(1, L):
            l = lax.rem(me + r, L)
            pltpu.make_async_remote_copy(
                src_ref=res.at[o, f, l],
                dst_ref=ret.at[o, f, me],
                send_sem=r_send,
                recv_sem=r_recv.at[o, f],
                device_id=dev_l(l),
                device_id_type=MESH,
            ).start()

    def expert(o):
        bytes_wait(disp.at[o, :, pl.ds(0, L - 1)], y_recv.at[o])
        gate_pre = jnp.zeros((L * CAP, gw.shape[1]), jnp.float32)
        up_pre = jnp.zeros((L * CAP, gw.shape[1]), jnp.float32)
        for f in range(S):
            block = recv[o, f].reshape(L * CAP, DS)
            cut = slice(f * DS, (f + 1) * DS)
            gate_pre += jnp.dot(block, gw[cut, :], preferred_element_type=jnp.float32)
            up_pre += jnp.dot(block, uw[cut, :], preferred_element_type=jnp.float32)
        act = clamped_unit(gate_pre, up_pre).astype(jnp.bfloat16)
        for f in range(S):
            cut = slice(f * DS, (f + 1) * DS)
            result = jnp.dot(act, dw[:, cut], preferred_element_type=jnp.float32)
            res[o, f] = result.astype(jnp.bfloat16).reshape(L, CAP, DS)
            ret[o, f, me] = res[o, f, me]

    def combine(o, f):
        bytes_wait(res.at[o, f, pl.ds(0, L - 1)], r_recv.at[o, f])
        block = ret[o, f].reshape(L * CAP, DS)
        return jnp.dot(spread[o, 0], block, preferred_element_type=jnp.float32) + jnp.dot(
            spread[o, 1], block, preferred_element_type=jnp.float32
        )

    def job_offset(k):
        h = (k + 1) // 2
        odd = lax.rem(k, 2)
        return odd * (Z - h) + (1 - odd) * h

    make_slots(0)
    for f in range(S):
        dispatch(0, f)

    loads[6].wait()

    def weight_copy(r):
        return pltpu.make_async_remote_copy(
            src_ref=wall.at[x],
            dst_ref=wall.at[x],
            send_sem=w_send,
            recv_sem=w_recv,
            device_id=dev_x(r),
            device_id_type=MESH,
        )

    for r in range(1, X):
        weight_copy(r).start()

    for load in loads[7:9]:
        load.wait()

    blocks = rows // WINDOW

    def attend(step, carry):
        b = blocks - 1 - step
        first = pl.multiple_of(b * WINDOW, WINDOW)
        keys = kv2[0, :, pl.ds(first, 2 * WINDOW)]
        vals = kv2[1, :, pl.ds(first, 2 * WINDOW)]
        qs = lax.broadcasted_iota(jnp.int32, (WINDOW, 2 * WINDOW), 0)
        ks = lax.broadcasted_iota(jnp.int32, (WINDOW, 2 * WINDOW), 1)
        lowest = jnp.where((ep == 0) & (b == 0), WINDOW, 0)
        valid = (ks > qs) & (ks <= qs + WINDOW) & (ks >= lowest)
        lower = lax.broadcasted_iota(jnp.int32, (WINDOW, 2 * HEAD_DIM), 1) < HEAD_DIM
        for pair in range(2):
            cut = slice(pair * 2 * HEAD_DIM, (pair + 1) * 2 * HEAD_DIM)
            both = q_ref[pl.ds(first, WINDOW), cut]
            halves = []
            for half in range(2):
                keep = lower if half == 0 else jnp.logical_not(lower)
                mine = jnp.where(keep, both, jnp.zeros_like(both))
                scores = jnp.dot(mine, keys, preferred_element_type=jnp.float32) * HEAD_DIM ** (-0.5)
                scores = jnp.where(valid, scores, NEGATIVE)
                sink = sink_ref[2 * pair + half]
                maxima = jnp.maximum(jnp.max(scores, axis=-1, keepdims=True), sink)
                powers = jnp.exp(scores - maxima)
                total = jnp.sum(powers, axis=-1, keepdims=True) + jnp.exp(sink - maxima)
                weights = (powers / total).astype(jnp.bfloat16)
                halves.append(
                    lax.dot_general(
                        weights, vals, (((1,), (1,)), ((), ())), preferred_element_type=jnp.float32
                    )
                )
            done = jnp.where(lower, halves[0], halves[1]).astype(jnp.bfloat16)
            heads[
                b * WINDOW // per_x, pl.ds(pl.multiple_of(lax.rem(b * WINDOW, per_x), WINDOW), WINDOW), cut
            ] = done
        return carry

    lax.fori_loop(0, blocks - 1, attend, 0)

    def finish_heads():
        halo.wait_recv()
        attend(blocks - 1, 0)
        hall[x] = heads[x]
        for r in range(1, X):
            send_heads(r)

    def send_heads(r):
        pltpu.make_async_remote_copy(
            src_ref=heads.at[lax.rem(x + r, X)],
            dst_ref=hall.at[x],
            send_sem=h_send,
            recv_sem=h_recv,
            device_id=dev_x(r),
            device_id_type=MESH,
        ).start()

    for load in loads[9:]:
        load.wait()

    def spread_step(u, carry):
        hop, i = u // S + 1, lax.rem(u, S)
        for direction in range(2):
            ring_copy(direction, u).wait_recv()

            @pl.when(u + S < U)
            def _():
                ring_copy(direction, u + S).start()

        @pl.when(i == 0)
        def _():
            bytes_wait(tab.at[0], tab_recv.at[Z - hop])

            @pl.when(hop < H)
            def _():
                tab_copy(0, hop + 1).start()
                bytes_wait(tab.at[0], tab_recv.at[hop])
                make_slots(hop)

            @pl.when(hop < H - 1)
            def _():
                tab_copy(1, hop + 1).start()

            make_slots(Z - hop)


        @pl.when((u < S - LATE) | (u >= S))
        def _():
            dispatch(Z - hop, i)
            dispatch(hop, S - 1 - i)

        half = S // 2
        k = u // half - 2

        @pl.when((lax.rem(u, half) == 0) & (k >= 3))
        def _():
            expert(job_offset(k))

        @pl.when(u == S - 1)
        def _():
            finish_heads()

        return carry

    lax.fori_loop(0, U, spread_step, 0)

    def back_unit(u):
        hop, i = u // S + 1, lax.rem(u, S)
        give_back(Z - hop, i)
        give_back(hop, S - 1 - i)

    first_late = max(3, Z - 3)

    def late_job(k, carry):
        expert(job_offset(k))

        @pl.when(k == Z - 2)
        def _():
            for u in range(S - LATE, S):
                dispatch(Z - 1, u)
                dispatch(1, S - 1 - u)

        return carry

    lax.fori_loop(first_late, Z, late_job, 0)

    ahead = min(AHEAD, U)
    for j in range(ahead):
        back_unit(U - 1 - j)

    def rs_copy(direction, u):
        return pltpu.make_async_remote_copy(
            src_ref=rs_out.at[direction, u],
            dst_ref=rs_in.at[direction, u],
            send_sem=rs_send.at[direction],
            recv_sem=rs_recv.at[direction, u],
            device_id=dev_z(1 if direction == 0 else -1),
            device_id_type=MESH,
        )

    for direction in range(2):
        for u in range(U, U + S):
            rs_in[direction, u] = jnp.zeros((T, DS), jnp.bfloat16)

    def gather_step(v, carry):
        u = U - 1 - v
        hop, i = u // S + 1, lax.rem(u, S)

        @pl.when(u >= ahead)
        def _():
            back_unit(u - ahead)

        @pl.when(v == U - 1 - S - ahead)
        def _():
            expert(0)

        @pl.when((v >= U - 3 - S - ahead) & (v < U - 1 - S - ahead))
        def _():
            expert(lax.rem((v - (U - 3 - S - ahead)) * 2 + Z - 1, Z))

        @pl.when(u == ahead - 1)
        def _():
            for f in range(S):
                give_back(0, f)

        for direction in range(2):
            o, f = (hop, S - 1 - i) if direction == 0 else (Z - hop, i)
            value = combine(o, f)

            @pl.when(u + S < U)
            def _():
                rs_copy(direction, u + S).wait_recv()

            value = value + rs_in[direction, u + S].astype(jnp.float32)
            rs_out[direction, u] = value.astype(jnp.bfloat16)
            rs_copy(direction, u).start()

        first = U // 2
        wide = att_ref.shape[1] // 4

        @pl.when(v == first)
        def _():
            bytes_wait(wall.at[pl.ds(0, X - 1)], w_recv)
            bytes_wait(hall.at[pl.ds(0, X - 1)], h_recv)

        @pl.when((v >= first) & (v < first + 4))
        def _():
            cut = pl.ds(pl.multiple_of((v - first) * wide, wide), wide)
            total = jnp.dot(hall[0], wall[0, :, cut], preferred_element_type=jnp.float32)
            for s in range(1, X):
                total += jnp.dot(hall[s], wall[s, :, cut], preferred_element_type=jnp.float32)
            att_ref[:, cut] = total.astype(jnp.bfloat16)

        return carry

    lax.fori_loop(0, U, gather_step, 0)

    for f in range(S):
        value = combine(0, f)
        rs_copy(0, S - 1 - f).wait_recv()
        rs_copy(1, f).wait_recv()
        value = value + rs_in[0, S - 1 - f].astype(jnp.float32) + rs_in[1, f].astype(jnp.float32)
        cut = slice(f * DS, (f + 1) * DS)
        out_ref[:, cut] = value.astype(jnp.bfloat16)

    bytes_wait(tab.at[pl.ds(0, Z - 1)], tab_send)
    for direction in range(2):
        bytes_wait(rs_in.at[direction, pl.ds(0, U)], z_send.at[direction])
        bytes_wait(rs_in.at[direction, pl.ds(0, U)], rs_send.at[direction])
    bytes_wait(disp.at[:, :, pl.ds(0, L - 1)], y_send)
    bytes_wait(res.at[:, :, pl.ds(0, L - 1)], r_send)
    bytes_wait(wall.at[pl.ds(0, X - 1)], w_send)
    bytes_wait(heads.at[pl.ds(0, X - 1)], h_send)
    halo.wait_send()


def on_device(
    Z,
    L,
    X,
    queries,
    head_keys,
    head_values,
    sink_logits,
    out_weight,
    moe_input,
    norm_gain,
    routes,
    route_weight,
    gate_weight,
    up_weight,
    down_weight,
):
    S = PIECES
    T, D = moe_input.shape
    DS = D // S
    FF = gate_weight.shape[2]
    rows, cols = queries.shape
    H = Z // 2
    U = (H - 1) * S + S // 2
    slots = L * CAP
    bf16, f32 = jnp.bfloat16, jnp.float32
    hbm = pl.BlockSpec(memory_space=pl.ANY)
    dma = pltpu.SemaphoreType.DMA
    attention_out, routed_out = pl.pallas_call(
        functools.partial(kernel, Z, L, X, S),
        out_shape=(
            pltpu.VMEM((rows // X, D), bf16),
            pltpu.VMEM((T, D), bf16),
        ),
        in_specs=[hbm] * 12,
        out_specs=(pl.BlockSpec(memory_space=pltpu.VMEM),) * 2,
        scratch_shapes=[
            pltpu.VMEM((T, D), bf16),
            pltpu.VMEM((1, D), f32),
            pltpu.VMEM(routes.shape[::-1], jnp.int32),
            pltpu.VMEM(routes.shape[::-1], f32),
            pltpu.VMEM((rows, cols), bf16),
            pltpu.VMEM((HEAD_DIM, rows), bf16),
            pltpu.VMEM((HEAD_DIM, rows), bf16),
            pltpu.SMEM(sink_logits.shape, f32),
            pltpu.VMEM((Z, S, T, DS), bf16),
            pltpu.VMEM((Z, 8, T), f32),
            pltpu.VMEM((Z, slots, T), bf16),
            pltpu.VMEM((Z, 2, T, slots), bf16),
            pltpu.VMEM((Z, S, L, CAP, DS), bf16),
            pltpu.VMEM((Z, S, L, CAP, DS), bf16),
            pltpu.VMEM((Z, S, L, CAP, DS), bf16),
            pltpu.VMEM((Z, S, L, CAP, DS), bf16),
            pltpu.VMEM((2, U, T, DS), bf16),
            pltpu.VMEM((2, U + S, T, DS), bf16),
            pltpu.VMEM((D, FF), bf16),
            pltpu.VMEM((D, FF), bf16),
            pltpu.VMEM((FF, D), bf16),
            pltpu.VMEM((X, cols, D), bf16),
            pltpu.VMEM((2, 2 * HEAD_DIM, rows + WINDOW), bf16),
            pltpu.VMEM((X, rows // X, cols), bf16),
            pltpu.VMEM((X, rows // X, cols), bf16),
            dma((12,)),
            dma,
            dma((Z,)),
            dma((2,)),
            dma((2, U)),
            dma,
            dma((Z,)),
            dma,
            dma((Z, S)),
            dma((2,)),
            dma((2, U)),
            dma,
            dma,
            dma,
            dma,
            dma,
            dma,
        ],
        compiler_params=pltpu.CompilerParams(
            collective_id=0, has_side_effects=True, vmem_limit_bytes=60 * 1024 * 1024
        ),
    )(
        moe_input,
        norm_gain.reshape(1, D),
        routes.T,
        route_weight.T,
        queries,
        head_keys.T,
        head_values.T,
        sink_logits,
        out_weight,
        gate_weight,
        up_weight,
        down_weight,
    )
    return write_out(attention_out, routed_out)


def write_out(*arrays):
    def body(*refs):
        copies = [pltpu.make_async_copy(refs[n], refs[2 + n], refs[4].at[n]) for n in range(2)]
        for copy in copies:
            copy.start()
        for copy in copies:
            copy.wait()

    return pl.pallas_call(
        body,
        out_shape=tuple(jax.ShapeDtypeStruct(a.shape, a.dtype) for a in arrays),
        in_specs=[pl.BlockSpec(memory_space=pltpu.VMEM)] * 2,
        out_specs=(pl.BlockSpec(memory_space=pl.ANY),) * 2,
        scratch_shapes=[pltpu.SemaphoreType.DMA((2,))],
    )(*[pltpu.with_memory_space_constraint(a, pltpu.VMEM) for a in arrays])


def solution(mesh, layer=8):
    X = mesh.shape["tp"]
    Z = mesh.shape["ep"] // layer
    placed = (
        P("ep", "tp"),
        P("ep", "tp"),
        P("ep", "tp"),
        P("tp"),
        P("tp", None),
        P(("ep", "tp"), None),
        P(),
        P(("ep", "tp"), None),
        P(("ep", "tp"), None),
        P("ep", None, None),
        P("ep", None, None),
        P("ep", None, None),
    )
    return jax.shard_map(
        functools.partial(on_device, Z, layer, X),
        mesh=mesh,
        in_specs=placed,
        out_specs=(P(("ep", "tp"), None), P(("ep", "tp"), None)),
        check_vma=False,
    )
```

```python
import functools

import jax
import jax.numpy as jnp
from jax import lax
from jax.experimental import pallas as pl
from jax.experimental.pallas import tpu as pltpu
from jax.sharding import PartitionSpec as P

MESH = pl.DeviceIdType.MESH
HEAD_DIM = 64
WINDOW = 128
CAP = 16
EPSILON = 1e-05
NEGATIVE = -1e30
PIECES = 8
AHEAD = 6
LATE = 1
OWN = 2


def clamped_unit(gate_pre, up_pre):
    gate_cut = jnp.minimum(gate_pre, 7.0)
    up_cut = jnp.clip(up_pre, -7.0, 7.0)
    return gate_cut * jax.nn.sigmoid(1.702 * gate_cut) * (up_cut + 1.0)


def bytes_wait(ref, sem):
    if 0 in ref.shape:
        return
    pltpu.make_async_copy(ref, ref, sem).wait()


def kernel(
    Z,
    L,
    X,
    S,
    x_hbm,
    gain_hbm,
    routes_hbm,
    rweight_hbm,
    q_hbm,
    k_hbm,
    v_hbm,
    sink_hbm,
    ow_hbm,
    gw_hbm,
    uw_hbm,
    dw_hbm,
    att_ref,
    out_ref,
    x_ref,
    gain_ref,
    routes_ref,
    rweight_ref,
    q_ref,
    k_ref,
    v_ref,
    sink_ref,
    ag,
    tab,
    pick,
    spread,
    disp,
    recv,
    res,
    ret,
    rs_out,
    rs_in,
    gw,
    uw,
    dw,
    wall,
    kv2,
    heads,
    hall,
    ld_sem,
    tab_send,
    tab_recv,
    z_send,
    z_recv,
    y_send,
    y_recv,
    r_send,
    r_recv,
    rs_send,
    rs_recv,
    w_send,
    w_recv,
    h_send,
    h_recv,
    halo_send,
    halo_recv,
):
    T, D = x_ref.shape
    DS = D // S
    H = Z // 2
    U = (H - 1) * S + S // 2
    EP = Z * L
    rows = q_ref.shape[0]
    per_x = rows // X
    ep = lax.axis_index("ep")
    x = lax.axis_index("tp")
    z = ep // L
    me = lax.rem(ep, L)

    def dev_z(step):
        return (lax.rem(z + step + Z, Z) * L + me, x)

    def dev_l(l):
        return (z * L + l, x)

    def dev_x(step):
        return (ep, lax.rem(x + step, X))

    right_ep = (lax.rem(ep + 1, EP), x)
    left_ep = (lax.rem(ep + EP - 1, EP), x)

    pairs = [
        (x_hbm, x_ref),
        (gain_hbm, gain_ref),
        (routes_hbm, routes_ref),
        (rweight_hbm, rweight_ref),
        (k_hbm, k_ref),
        (v_hbm, v_ref),
        (ow_hbm, wall.at[x]),
        (q_hbm, q_ref),
        (sink_hbm, sink_ref),
        (gw_hbm.at[0], gw),
        (uw_hbm.at[0], uw),
        (dw_hbm.at[0], dw),
    ]
    loads = [pltpu.make_async_copy(a, b, ld_sem.at[n]) for n, (a, b) in enumerate(pairs)]
    barrier = pltpu.get_barrier_semaphore()
    met = [dev_z(1), dev_z(-1)]
    met += [dev_l(lax.rem(me + r, L)) for r in range(1, L)]
    met += [dev_x(r) for r in range(1, X)]
    met += [right_ep, left_ep]
    for target in met:
        pl.semaphore_signal(barrier, inc=1, device_id=target, device_id_type=MESH)
    for load in loads[:6]:
        load.start()

    for load in loads[:2]:
        load.wait()
    values32 = x_ref[...].astype(jnp.float32)
    scale = lax.rsqrt(jnp.mean(values32 * values32, axis=-1, keepdims=True) + EPSILON)
    normed = (values32 * scale * gain_ref[...]).astype(jnp.bfloat16)
    for f in range(S):
        ag[0, f] = normed[:, f * DS : (f + 1) * DS]
    for load in loads[2:6]:
        load.wait()
    for load in loads[6:]:
        load.start()
    tab[0, 0:4] = routes_ref[...].astype(jnp.float32)
    tab[0, 4:8] = rweight_ref[...]
    for half in range(2):
        cut = slice(half * HEAD_DIM, (half + 1) * HEAD_DIM)
        kv2[0, cut, WINDOW:] = k_ref[...]
        kv2[1, cut, WINDOW:] = v_ref[...]

    pl.semaphore_wait(barrier, len(met))

    halo = pltpu.make_async_remote_copy(
        src_ref=kv2.at[:, :, pl.ds(rows, WINDOW)],
        dst_ref=kv2.at[:, :, pl.ds(0, WINDOW)],
        send_sem=halo_send,
        recv_sem=halo_recv,
        device_id=right_ep,
        device_id_type=MESH,
    )
    halo.start()

    def tab_copy(direction, hop):
        if direction == 0:
            src, dst, target = lax.rem(Z - hop + 1, Z), Z - hop, dev_z(1)
        else:
            src, dst, target = hop - 1, hop, dev_z(-1)
        return pltpu.make_async_remote_copy(
            src_ref=tab.at[src],
            dst_ref=tab.at[dst],
            send_sem=tab_send,
            recv_sem=tab_recv.at[dst],
            device_id=target,
            device_id_type=MESH,
        )

    tab_copy(0, 1).start()
    if H > 1:
        tab_copy(1, 1).start()

    def ring_copy(direction, u):
        hop, i = u // S + 1, lax.rem(u, S)
        if direction == 0:
            f, src, dst, target = i, lax.rem(Z - hop + 1, Z), Z - hop, dev_z(1)
        else:
            f, src, dst, target = S - 1 - i, hop - 1, hop, dev_z(-1)
        return pltpu.make_async_remote_copy(
            src_ref=ag.at[src, f],
            dst_ref=ag.at[dst, f],
            send_sem=z_send.at[direction],
            recv_sem=z_recv.at[direction, u],
            device_id=target,
            device_id_type=MESH,
        )

    for u in range(min(S, U)):
        ring_copy(0, u).start()
        ring_copy(1, u).start()

    def make_slots(o):
        table = tab[o]
        expert = (lax.broadcasted_iota(jnp.int32, (L, T), 0) + z * L).astype(jnp.float32)
        named = jnp.zeros((L, T), jnp.float32)
        weight = jnp.zeros((L, T), jnp.float32)
        for k in range(4):
            hit = table[k : k + 1, :] == expert
            named = named + jnp.where(hit, 1.0, 0.0)
            weight = weight + jnp.where(hit, table[4 + k : 5 + k, :], 0.0)
        before = (
            lax.broadcasted_iota(jnp.int32, (T, T), 0) < lax.broadcasted_iota(jnp.int32, (T, T), 1)
        ).astype(jnp.float32)
        rank = jnp.dot(named, before, preferred_element_type=jnp.float32)
        rank = jnp.where(named > 0.5, rank, -1.0)
        slot = lax.broadcasted_iota(jnp.int32, (CAP, T), 0).astype(jnp.float32)
        hits = jnp.concatenate(
            [jnp.where(rank[l : l + 1, :] == slot, 1.0, 0.0) for l in range(L)], axis=0
        )
        weights = jnp.concatenate(
            [jnp.where(rank[l : l + 1, :] == slot, weight[l : l + 1, :], 0.0) for l in range(L)],
            axis=0,
        )
        pick[o] = hits.astype(jnp.bfloat16)
        turned = weights.T
        high = turned.astype(jnp.bfloat16)
        spread[o, 0] = high
        spread[o, 1] = (turned - high.astype(jnp.float32)).astype(jnp.bfloat16)

    def dispatch(o, f):
        chosen = jnp.dot(pick[o], ag[o, f], preferred_element_type=jnp.float32)
        disp[o, f] = chosen.astype(jnp.bfloat16).reshape(L, CAP, DS)
        recv[o, f, me] = disp[o, f, me]
        for r in range(1, L):
            l = lax.rem(me + r, L)
            pltpu.make_async_remote_copy(
                src_ref=disp.at[o, f, l],
                dst_ref=recv.at[o, f, me],
                send_sem=y_send,
                recv_sem=y_recv.at[o],
                device_id=dev_l(l),
                device_id_type=MESH,
            ).start()

    def give_back(o, f):
        for r in range(1, L):
            l = lax.rem(me + r, L)
            pltpu.make_async_remote_copy(
                src_ref=res.at[o, f, l],
                dst_ref=ret.at[o, f, me],
                send_sem=r_send,
                recv_sem=r_recv.at[o, f],
                device_id=dev_l(l),
                device_id_type=MESH,
            ).start()

    def expert(o):
        bytes_wait(disp.at[o, :, pl.ds(0, L - 1)], y_recv.at[o])
        gate_pre = jnp.zeros((L * CAP, gw.shape[1]), jnp.float32)
        up_pre = jnp.zeros((L * CAP, gw.shape[1]), jnp.float32)
        for f in range(S):
            block = recv[o, f].reshape(L * CAP, DS)
            cut = slice(f * DS, (f + 1) * DS)
            gate_pre += jnp.dot(block, gw[cut, :], preferred_element_type=jnp.float32)
            up_pre += jnp.dot(block, uw[cut, :], preferred_element_type=jnp.float32)
        act = clamped_unit(gate_pre, up_pre).astype(jnp.bfloat16)
        for f in range(S):
            cut = slice(f * DS, (f + 1) * DS)
            result = jnp.dot(act, dw[:, cut], preferred_element_type=jnp.float32)
            res[o, f] = result.astype(jnp.bfloat16).reshape(L, CAP, DS)
            ret[o, f, me] = res[o, f, me]

    def combine(o, f):
        bytes_wait(res.at[o, f, pl.ds(0, L - 1)], r_recv.at[o, f])
        block = ret[o, f].reshape(L * CAP, DS)
        return jnp.dot(spread[o, 0], block, preferred_element_type=jnp.float32) + jnp.dot(
            spread[o, 1], block, preferred_element_type=jnp.float32
        )

    def job_offset(k):
        h = (k + 1) // 2
        odd = lax.rem(k, 2)
        return odd * (Z - h) + (1 - odd) * h

    make_slots(0)
    for f in range(S):
        dispatch(0, f)

    loads[6].wait()

    def weight_copy(r):
        return pltpu.make_async_remote_copy(
            src_ref=wall.at[x],
            dst_ref=wall.at[x],
            send_sem=w_send,
            recv_sem=w_recv,
            device_id=dev_x(r),
            device_id_type=MESH,
        )

    for r in range(1, X):
        weight_copy(r).start()

    for load in loads[7:9]:
        load.wait()

    blocks = rows // WINDOW

    def attend(step, carry):
        b = blocks - 1 - step
        first = pl.multiple_of(b * WINDOW, WINDOW)
        keys = kv2[0, :, pl.ds(first, 2 * WINDOW)]
        vals = kv2[1, :, pl.ds(first, 2 * WINDOW)]
        qs = lax.broadcasted_iota(jnp.int32, (WINDOW, 2 * WINDOW), 0)
        ks = lax.broadcasted_iota(jnp.int32, (WINDOW, 2 * WINDOW), 1)
        lowest = jnp.where((ep == 0) & (b == 0), WINDOW, 0)
        valid = (ks > qs) & (ks <= qs + WINDOW) & (ks >= lowest)
        lower = lax.broadcasted_iota(jnp.int32, (WINDOW, 2 * HEAD_DIM), 1) < HEAD_DIM
        for pair in range(2):
            cut = slice(pair * 2 * HEAD_DIM, (pair + 1) * 2 * HEAD_DIM)
            both = q_ref[pl.ds(first, WINDOW), cut]
            halves = []
            for half in range(2):
                keep = lower if half == 0 else jnp.logical_not(lower)
                mine = jnp.where(keep, both, jnp.zeros_like(both))
                scores = jnp.dot(mine, keys, preferred_element_type=jnp.float32) * HEAD_DIM ** (-0.5)
                scores = jnp.where(valid, scores, NEGATIVE)
                sink = sink_ref[2 * pair + half]
                maxima = jnp.maximum(jnp.max(scores, axis=-1, keepdims=True), sink)
                powers = jnp.exp(scores - maxima)
                total = jnp.sum(powers, axis=-1, keepdims=True) + jnp.exp(sink - maxima)
                weights = (powers / total).astype(jnp.bfloat16)
                halves.append(
                    lax.dot_general(
                        weights, vals, (((1,), (1,)), ((), ())), preferred_element_type=jnp.float32
                    )
                )
            done = jnp.where(lower, halves[0], halves[1]).astype(jnp.bfloat16)
            heads[
                b * WINDOW // per_x, pl.ds(pl.multiple_of(lax.rem(b * WINDOW, per_x), WINDOW), WINDOW), cut
            ] = done
        return carry

    lax.fori_loop(0, blocks - 1, attend, 0)

    def finish_heads():
        halo.wait_recv()
        attend(blocks - 1, 0)
        hall[x] = heads[x]
        for r in range(1, X):
            send_heads(r)

    def send_heads(r):
        pltpu.make_async_remote_copy(
            src_ref=heads.at[lax.rem(x + r, X)],
            dst_ref=hall.at[x],
            send_sem=h_send,
            recv_sem=h_recv,
            device_id=dev_x(r),
            device_id_type=MESH,
        ).start()

    for load in loads[9:]:
        load.wait()

    def spread_step(u, carry):
        hop, i = u // S + 1, lax.rem(u, S)
        for direction in range(2):
            ring_copy(direction, u).wait_recv()

            @pl.when(u + S < U)
            def _():
                ring_copy(direction, u + S).start()

        @pl.when(i == 0)
        def _():
            bytes_wait(tab.at[0], tab_recv.at[Z - hop])

            @pl.when(hop < H)
            def _():
                tab_copy(0, hop + 1).start()
                bytes_wait(tab.at[0], tab_recv.at[hop])
                make_slots(hop)

            @pl.when(hop < H - 1)
            def _():
                tab_copy(1, hop + 1).start()

            make_slots(Z - hop)


        @pl.when((u < S - LATE) | (u >= S))
        def _():
            dispatch(Z - hop, i)
            dispatch(hop, S - 1 - i)

        half = S // 2
        k = u // half - 2

        @pl.when((lax.rem(u, half) == 0) & (k >= 3))
        def _():
            expert(job_offset(k))

        @pl.when(u == S - 1)
        def _():
            finish_heads()

        return carry

    lax.fori_loop(0, U, spread_step, 0)

    def back_unit(u):
        hop, i = u // S + 1, lax.rem(u, S)
        give_back(Z - hop, i)
        give_back(hop, S - 1 - i)

    first_late = max(3, Z - 3)

    def late_job(k, carry):
        expert(job_offset(k))

        @pl.when(k == Z - 2)
        def _():
            for u in range(S - LATE, S):
                dispatch(Z - 1, u)
                dispatch(1, S - 1 - u)
            expert(0)
            for f in range(OWN):
                give_back(0, f)

        return carry

    lax.fori_loop(first_late, Z, late_job, 0)

    ahead = min(AHEAD, U)
    for j in range(ahead):
        back_unit(U - 1 - j)

    def rs_copy(direction, u):
        return pltpu.make_async_remote_copy(
            src_ref=rs_out.at[direction, u],
            dst_ref=rs_in.at[direction, u],
            send_sem=rs_send.at[direction],
            recv_sem=rs_recv.at[direction, u],
            device_id=dev_z(1 if direction == 0 else -1),
            device_id_type=MESH,
        )

    for direction in range(2):
        for u in range(U, U + S):
            rs_in[direction, u] = jnp.zeros((T, DS), jnp.bfloat16)

    def gather_step(v, carry):
        u = U - 1 - v
        hop, i = u // S + 1, lax.rem(u, S)

        @pl.when(u >= ahead)
        def _():
            back_unit(u - ahead)

        @pl.when((v >= U - 3 - S - ahead) & (v < U - 1 - S - ahead))
        def _():
            expert(lax.rem((v - (U - 3 - S - ahead)) * 2 + Z - 1, Z))

        @pl.when(u == ahead - 1)
        def _():
            for f in range(OWN, S):
                give_back(0, f)

        for direction in range(2):
            o, f = (hop, S - 1 - i) if direction == 0 else (Z - hop, i)
            value = combine(o, f)

            @pl.when(u + S < U)
            def _():
                rs_copy(direction, u + S).wait_recv()

            value = value + rs_in[direction, u + S].astype(jnp.float32)
            rs_out[direction, u] = value.astype(jnp.bfloat16)
            rs_copy(direction, u).start()

        first = U // 2
        wide = att_ref.shape[1] // 4

        @pl.when(v == first)
        def _():
            bytes_wait(wall.at[pl.ds(0, X - 1)], w_recv)
            bytes_wait(hall.at[pl.ds(0, X - 1)], h_recv)

        @pl.when((v >= first) & (v < first + 4))
        def _():
            cut = pl.ds(pl.multiple_of((v - first) * wide, wide), wide)
            total = jnp.dot(hall[0], wall[0, :, cut], preferred_element_type=jnp.float32)
            for s in range(1, X):
                total += jnp.dot(hall[s], wall[s, :, cut], preferred_element_type=jnp.float32)
            att_ref[:, cut] = total.astype(jnp.bfloat16)

        return carry

    lax.fori_loop(0, U, gather_step, 0)

    for f in range(S):
        value = combine(0, f)
        rs_copy(0, S - 1 - f).wait_recv()
        rs_copy(1, f).wait_recv()
        value = value + rs_in[0, S - 1 - f].astype(jnp.float32) + rs_in[1, f].astype(jnp.float32)
        cut = slice(f * DS, (f + 1) * DS)
        out_ref[:, cut] = value.astype(jnp.bfloat16)

    bytes_wait(tab.at[pl.ds(0, Z - 1)], tab_send)
    for direction in range(2):
        bytes_wait(rs_in.at[direction, pl.ds(0, U)], z_send.at[direction])
        bytes_wait(rs_in.at[direction, pl.ds(0, U)], rs_send.at[direction])
    bytes_wait(disp.at[:, :, pl.ds(0, L - 1)], y_send)
    bytes_wait(res.at[:, :, pl.ds(0, L - 1)], r_send)
    bytes_wait(wall.at[pl.ds(0, X - 1)], w_send)
    bytes_wait(heads.at[pl.ds(0, X - 1)], h_send)
    halo.wait_send()


def on_device(
    Z,
    L,
    X,
    queries,
    head_keys,
    head_values,
    sink_logits,
    out_weight,
    moe_input,
    norm_gain,
    routes,
    route_weight,
    gate_weight,
    up_weight,
    down_weight,
):
    S = PIECES
    T, D = moe_input.shape
    DS = D // S
    FF = gate_weight.shape[2]
    rows, cols = queries.shape
    H = Z // 2
    U = (H - 1) * S + S // 2
    slots = L * CAP
    bf16, f32 = jnp.bfloat16, jnp.float32
    hbm = pl.BlockSpec(memory_space=pl.ANY)
    dma = pltpu.SemaphoreType.DMA
    attention_out, routed_out = pl.pallas_call(
        functools.partial(kernel, Z, L, X, S),
        out_shape=(
            pltpu.VMEM((rows // X, D), bf16),
            pltpu.VMEM((T, D), bf16),
        ),
        in_specs=[hbm] * 12,
        out_specs=(pl.BlockSpec(memory_space=pltpu.VMEM),) * 2,
        scratch_shapes=[
            pltpu.VMEM((T, D), bf16),
            pltpu.VMEM((1, D), f32),
            pltpu.VMEM(routes.shape[::-1], jnp.int32),
            pltpu.VMEM(routes.shape[::-1], f32),
            pltpu.VMEM((rows, cols), bf16),
            pltpu.VMEM((HEAD_DIM, rows), bf16),
            pltpu.VMEM((HEAD_DIM, rows), bf16),
            pltpu.SMEM(sink_logits.shape, f32),
            pltpu.VMEM((Z, S, T, DS), bf16),
            pltpu.VMEM((Z, 8, T), f32),
            pltpu.VMEM((Z, slots, T), bf16),
            pltpu.VMEM((Z, 2, T, slots), bf16),
            pltpu.VMEM((Z, S, L, CAP, DS), bf16),
            pltpu.VMEM((Z, S, L, CAP, DS), bf16),
            pltpu.VMEM((Z, S, L, CAP, DS), bf16),
            pltpu.VMEM((Z, S, L, CAP, DS), bf16),
            pltpu.VMEM((2, U, T, DS), bf16),
            pltpu.VMEM((2, U + S, T, DS), bf16),
            pltpu.VMEM((D, FF), bf16),
            pltpu.VMEM((D, FF), bf16),
            pltpu.VMEM((FF, D), bf16),
            pltpu.VMEM((X, cols, D), bf16),
            pltpu.VMEM((2, 2 * HEAD_DIM, rows + WINDOW), bf16),
            pltpu.VMEM((X, rows // X, cols), bf16),
            pltpu.VMEM((X, rows // X, cols), bf16),
            dma((12,)),
            dma,
            dma((Z,)),
            dma((2,)),
            dma((2, U)),
            dma,
            dma((Z,)),
            dma,
            dma((Z, S)),
            dma((2,)),
            dma((2, U)),
            dma,
            dma,
            dma,
            dma,
            dma,
            dma,
        ],
        compiler_params=pltpu.CompilerParams(
            collective_id=0, has_side_effects=True, vmem_limit_bytes=60 * 1024 * 1024
        ),
    )(
        moe_input,
        norm_gain.reshape(1, D),
        routes.T,
        route_weight.T,
        queries,
        head_keys.T,
        head_values.T,
        sink_logits,
        out_weight,
        gate_weight,
        up_weight,
        down_weight,
    )
    return write_out(attention_out, routed_out)


def write_out(*arrays):
    def body(*refs):
        copies = [pltpu.make_async_copy(refs[n], refs[2 + n], refs[4].at[n]) for n in range(2)]
        for copy in copies:
            copy.start()
        for copy in copies:
            copy.wait()

    return pl.pallas_call(
        body,
        out_shape=tuple(jax.ShapeDtypeStruct(a.shape, a.dtype) for a in arrays),
        in_specs=[pl.BlockSpec(memory_space=pltpu.VMEM)] * 2,
        out_specs=(pl.BlockSpec(memory_space=pl.ANY),) * 2,
        scratch_shapes=[pltpu.SemaphoreType.DMA((2,))],
    )(*[pltpu.with_memory_space_constraint(a, pltpu.VMEM) for a in arrays])


def solution(mesh, layer=8):
    X = mesh.shape["tp"]
    Z = mesh.shape["ep"] // layer
    placed = (
        P("ep", "tp"),
        P("ep", "tp"),
        P("ep", "tp"),
        P("tp"),
        P("tp", None),
        P(("ep", "tp"), None),
        P(),
        P(("ep", "tp"), None),
        P(("ep", "tp"), None),
        P("ep", None, None),
        P("ep", None, None),
        P("ep", None, None),
    )
    return jax.shard_map(
        functools.partial(on_device, Z, layer, X),
        mesh=mesh,
        in_specs=placed,
        out_specs=(P(("ep", "tp"), None), P(("ep", "tp"), None)),
        check_vma=False,
    )
```

```python
import functools

import jax
import jax.numpy as jnp
from jax import lax
from jax.experimental import pallas as pl
from jax.experimental.pallas import tpu as pltpu
from jax.sharding import PartitionSpec as P

MESH = pl.DeviceIdType.MESH
HEAD_DIM = 64
WINDOW = 128
CAP = 16
EPSILON = 1e-05
NEGATIVE = -1e30
PIECES = 8
AHEAD = 6
LATE = 1
OWN = 2


def clamped_unit(gate_pre, up_pre):
    gate_cut = jnp.minimum(gate_pre, 7.0)
    up_cut = jnp.clip(up_pre, -7.0, 7.0)
    return gate_cut * jax.nn.sigmoid(1.702 * gate_cut) * (up_cut + 1.0)


def bytes_wait(ref, sem):
    if 0 in ref.shape:
        return
    pltpu.make_async_copy(ref, ref, sem).wait()


def kernel(
    Z,
    L,
    X,
    S,
    x_hbm,
    gain_hbm,
    routes_hbm,
    rweight_hbm,
    q_hbm,
    k_hbm,
    v_hbm,
    sink_hbm,
    ow_hbm,
    gw_hbm,
    uw_hbm,
    dw_hbm,
    att_ref,
    out_ref,
    x_ref,
    gain_ref,
    routes_ref,
    rweight_ref,
    q_ref,
    k_ref,
    v_ref,
    sink_ref,
    ag,
    tab,
    pick,
    spread,
    disp,
    recv,
    res,
    ret,
    rs_out,
    rs_in,
    gw,
    uw,
    dw,
    wall,
    kv2,
    heads,
    hall,
    ld_sem,
    tab_send,
    tab_recv,
    z_send,
    z_recv,
    y_send,
    y_recv,
    r_send,
    r_recv,
    rs_send,
    rs_recv,
    w_send,
    w_recv,
    h_send,
    h_recv,
    halo_send,
    halo_recv,
):
    T, D = x_ref.shape
    DS = D // S
    H = Z // 2
    U = (H - 1) * S + S // 2
    EP = Z * L
    rows = q_ref.shape[0]
    per_x = rows // X
    ep = lax.axis_index("ep")
    x = lax.axis_index("tp")
    z = ep // L
    me = lax.rem(ep, L)

    def dev_z(step):
        return (lax.rem(z + step + Z, Z) * L + me, x)

    def dev_l(l):
        return (z * L + l, x)

    def dev_x(step):
        return (ep, lax.rem(x + step, X))

    right_ep = (lax.rem(ep + 1, EP), x)
    left_ep = (lax.rem(ep + EP - 1, EP), x)

    pairs = [
        (x_hbm, x_ref),
        (gain_hbm, gain_ref),
        (routes_hbm, routes_ref),
        (rweight_hbm, rweight_ref),
        (k_hbm, k_ref),
        (v_hbm, v_ref),
        (ow_hbm, wall.at[x]),
        (q_hbm, q_ref),
        (sink_hbm, sink_ref),
        (gw_hbm.at[0], gw),
        (uw_hbm.at[0], uw),
        (dw_hbm.at[0], dw),
    ]
    loads = [pltpu.make_async_copy(a, b, ld_sem.at[n]) for n, (a, b) in enumerate(pairs)]
    barrier = pltpu.get_barrier_semaphore()
    met = [dev_z(1), dev_z(-1)]
    met += [dev_l(lax.rem(me + r, L)) for r in range(1, L)]
    met += [dev_x(r) for r in range(1, X)]
    met += [right_ep, left_ep]
    for target in met:
        pl.semaphore_signal(barrier, inc=1, device_id=target, device_id_type=MESH)
    for load in loads[:6]:
        load.start()

    for load in loads[:2]:
        load.wait()
    values32 = x_ref[...].astype(jnp.float32)
    scale = lax.rsqrt(jnp.mean(values32 * values32, axis=-1, keepdims=True) + EPSILON)
    normed = (values32 * scale * gain_ref[...]).astype(jnp.bfloat16)
    for f in range(S):
        ag[0, f] = normed[:, f * DS : (f + 1) * DS]
    pl.semaphore_wait(barrier, len(met))

    def ring_copy(direction, u):
        hop, i = u // S + 1, lax.rem(u, S)
        if direction == 0:
            f, src, dst, target = i, lax.rem(Z - hop + 1, Z), Z - hop, dev_z(1)
        else:
            f, src, dst, target = S - 1 - i, hop - 1, hop, dev_z(-1)
        return pltpu.make_async_remote_copy(
            src_ref=ag.at[src, f],
            dst_ref=ag.at[dst, f],
            send_sem=z_send.at[direction],
            recv_sem=z_recv.at[direction, u],
            device_id=target,
            device_id_type=MESH,
        )

    for u in range(2):
        ring_copy(0, u).start()
        ring_copy(1, u).start()

    for load in loads[2:6]:
        load.wait()
    for load in loads[6:]:
        load.start()
    tab[0, 0:4] = routes_ref[...].astype(jnp.float32)
    tab[0, 4:8] = rweight_ref[...]
    for half in range(2):
        cut = slice(half * HEAD_DIM, (half + 1) * HEAD_DIM)
        kv2[0, cut, WINDOW:] = k_ref[...]
        kv2[1, cut, WINDOW:] = v_ref[...]

    halo = pltpu.make_async_remote_copy(
        src_ref=kv2.at[:, :, pl.ds(rows, WINDOW)],
        dst_ref=kv2.at[:, :, pl.ds(0, WINDOW)],
        send_sem=halo_send,
        recv_sem=halo_recv,
        device_id=right_ep,
        device_id_type=MESH,
    )
    halo.start()

    def tab_copy(direction, hop):
        if direction == 0:
            src, dst, target = lax.rem(Z - hop + 1, Z), Z - hop, dev_z(1)
        else:
            src, dst, target = hop - 1, hop, dev_z(-1)
        return pltpu.make_async_remote_copy(
            src_ref=tab.at[src],
            dst_ref=tab.at[dst],
            send_sem=tab_send,
            recv_sem=tab_recv.at[dst],
            device_id=target,
            device_id_type=MESH,
        )

    tab_copy(0, 1).start()
    if H > 1:
        tab_copy(1, 1).start()

    for u in range(2, S):
        ring_copy(0, u).start()
        ring_copy(1, u).start()

    def make_slots(o):
        table = tab[o]
        expert = (lax.broadcasted_iota(jnp.int32, (L, T), 0) + z * L).astype(jnp.float32)
        named = jnp.zeros((L, T), jnp.float32)
        weight = jnp.zeros((L, T), jnp.float32)
        for k in range(4):
            hit = table[k : k + 1, :] == expert
            named = named + jnp.where(hit, 1.0, 0.0)
            weight = weight + jnp.where(hit, table[4 + k : 5 + k, :], 0.0)
        before = (
            lax.broadcasted_iota(jnp.int32, (T, T), 0) < lax.broadcasted_iota(jnp.int32, (T, T), 1)
        ).astype(jnp.float32)
        rank = jnp.dot(named, before, preferred_element_type=jnp.float32)
        rank = jnp.where(named > 0.5, rank, -1.0)
        slot = lax.broadcasted_iota(jnp.int32, (CAP, T), 0).astype(jnp.float32)
        hits = jnp.concatenate(
            [jnp.where(rank[l : l + 1, :] == slot, 1.0, 0.0) for l in range(L)], axis=0
        )
        weights = jnp.concatenate(
            [jnp.where(rank[l : l + 1, :] == slot, weight[l : l + 1, :], 0.0) for l in range(L)],
            axis=0,
        )
        pick[o] = hits.astype(jnp.bfloat16)
        turned = weights.T
        high = turned.astype(jnp.bfloat16)
        spread[o, 0] = high
        spread[o, 1] = (turned - high.astype(jnp.float32)).astype(jnp.bfloat16)

    def dispatch(o, f):
        chosen = jnp.dot(pick[o], ag[o, f], preferred_element_type=jnp.float32)
        disp[o, f] = chosen.astype(jnp.bfloat16).reshape(L, CAP, DS)
        recv[o, f, me] = disp[o, f, me]
        for r in range(1, L):
            l = lax.rem(me + r, L)
            pltpu.make_async_remote_copy(
                src_ref=disp.at[o, f, l],
                dst_ref=recv.at[o, f, me],
                send_sem=y_send,
                recv_sem=y_recv.at[o],
                device_id=dev_l(l),
                device_id_type=MESH,
            ).start()

    def give_back(o, f):
        for r in range(1, L):
            l = lax.rem(me + r, L)
            pltpu.make_async_remote_copy(
                src_ref=res.at[o, f, l],
                dst_ref=ret.at[o, f, me],
                send_sem=r_send,
                recv_sem=r_recv.at[o, f],
                device_id=dev_l(l),
                device_id_type=MESH,
            ).start()

    def expert(o):
        bytes_wait(disp.at[o, :, pl.ds(0, L - 1)], y_recv.at[o])
        gate_pre = jnp.zeros((L * CAP, gw.shape[1]), jnp.float32)
        up_pre = jnp.zeros((L * CAP, gw.shape[1]), jnp.float32)
        for f in range(S):
            block = recv[o, f].reshape(L * CAP, DS)
            cut = slice(f * DS, (f + 1) * DS)
            gate_pre += jnp.dot(block, gw[cut, :], preferred_element_type=jnp.float32)
            up_pre += jnp.dot(block, uw[cut, :], preferred_element_type=jnp.float32)
        act = clamped_unit(gate_pre, up_pre).astype(jnp.bfloat16)
        for f in range(S):
            cut = slice(f * DS, (f + 1) * DS)
            result = jnp.dot(act, dw[:, cut], preferred_element_type=jnp.float32)
            res[o, f] = result.astype(jnp.bfloat16).reshape(L, CAP, DS)
            ret[o, f, me] = res[o, f, me]

    def combine(o, f):
        bytes_wait(res.at[o, f, pl.ds(0, L - 1)], r_recv.at[o, f])
        block = ret[o, f].reshape(L * CAP, DS)
        return jnp.dot(spread[o, 0], block, preferred_element_type=jnp.float32) + jnp.dot(
            spread[o, 1], block, preferred_element_type=jnp.float32
        )

    def job_offset(k):
        h = (k + 1) // 2
        odd = lax.rem(k, 2)
        return odd * (Z - h) + (1 - odd) * h

    make_slots(0)
    for f in range(S):
        dispatch(0, f)

    loads[6].wait()

    def weight_copy(r):
        return pltpu.make_async_remote_copy(
            src_ref=wall.at[x],
            dst_ref=wall.at[x],
            send_sem=w_send,
            recv_sem=w_recv,
            device_id=dev_x(r),
            device_id_type=MESH,
        )

    for r in range(1, X):
        weight_copy(r).start()

    for load in loads[7:9]:
        load.wait()

    blocks = rows // WINDOW

    def attend(step, carry):
        b = blocks - 1 - step
        first = pl.multiple_of(b * WINDOW, WINDOW)
        keys = kv2[0, :, pl.ds(first, 2 * WINDOW)]
        vals = kv2[1, :, pl.ds(first, 2 * WINDOW)]
        qs = lax.broadcasted_iota(jnp.int32, (WINDOW, 2 * WINDOW), 0)
        ks = lax.broadcasted_iota(jnp.int32, (WINDOW, 2 * WINDOW), 1)
        lowest = jnp.where((ep == 0) & (b == 0), WINDOW, 0)
        valid = (ks > qs) & (ks <= qs + WINDOW) & (ks >= lowest)
        lower = lax.broadcasted_iota(jnp.int32, (WINDOW, 2 * HEAD_DIM), 1) < HEAD_DIM
        for pair in range(2):
            cut = slice(pair * 2 * HEAD_DIM, (pair + 1) * 2 * HEAD_DIM)
            both = q_ref[pl.ds(first, WINDOW), cut]
            halves = []
            for half in range(2):
                keep = lower if half == 0 else jnp.logical_not(lower)
                mine = jnp.where(keep, both, jnp.zeros_like(both))
                scores = jnp.dot(mine, keys, preferred_element_type=jnp.float32) * HEAD_DIM ** (-0.5)
                scores = jnp.where(valid, scores, NEGATIVE)
                sink = sink_ref[2 * pair + half]
                maxima = jnp.maximum(jnp.max(scores, axis=-1, keepdims=True), sink)
                powers = jnp.exp(scores - maxima)
                total = jnp.sum(powers, axis=-1, keepdims=True) + jnp.exp(sink - maxima)
                weights = (powers / total).astype(jnp.bfloat16)
                halves.append(
                    lax.dot_general(
                        weights, vals, (((1,), (1,)), ((), ())), preferred_element_type=jnp.float32
                    )
                )
            done = jnp.where(lower, halves[0], halves[1]).astype(jnp.bfloat16)
            heads[
                b * WINDOW // per_x, pl.ds(pl.multiple_of(lax.rem(b * WINDOW, per_x), WINDOW), WINDOW), cut
            ] = done
        return carry

    lax.fori_loop(0, blocks - 1, attend, 0)

    def finish_heads():
        halo.wait_recv()
        attend(blocks - 1, 0)
        hall[x] = heads[x]
        for r in range(1, X):
            send_heads(r)

    def send_heads(r):
        pltpu.make_async_remote_copy(
            src_ref=heads.at[lax.rem(x + r, X)],
            dst_ref=hall.at[x],
            send_sem=h_send,
            recv_sem=h_recv,
            device_id=dev_x(r),
            device_id_type=MESH,
        ).start()

    for load in loads[9:]:
        load.wait()

    def spread_step(u, carry):
        hop, i = u // S + 1, lax.rem(u, S)
        for direction in range(2):
            ring_copy(direction, u).wait_recv()

            @pl.when(u + S < U)
            def _():
                ring_copy(direction, u + S).start()

        @pl.when(i == 0)
        def _():
            bytes_wait(tab.at[0], tab_recv.at[Z - hop])

            @pl.when(hop < H)
            def _():
                tab_copy(0, hop + 1).start()
                bytes_wait(tab.at[0], tab_recv.at[hop])
                make_slots(hop)

            @pl.when(hop < H - 1)
            def _():
                tab_copy(1, hop + 1).start()

            make_slots(Z - hop)


        @pl.when((u < S - LATE) | (u >= S))
        def _():
            dispatch(Z - hop, i)
            dispatch(hop, S - 1 - i)

        half = S // 2
        k = u // half - 2

        @pl.when((lax.rem(u, half) == 0) & (k >= 3))
        def _():
            expert(job_offset(k))

        @pl.when(u == S - 1)
        def _():
            finish_heads()

        return carry

    lax.fori_loop(0, U, spread_step, 0)

    def back_unit(u):
        hop, i = u // S + 1, lax.rem(u, S)
        give_back(Z - hop, i)
        give_back(hop, S - 1 - i)

    first_late = max(3, Z - 3)

    def late_job(k, carry):
        expert(job_offset(k))

        @pl.when(k == Z - 2)
        def _():
            for u in range(S - LATE, S):
                dispatch(Z - 1, u)
                dispatch(1, S - 1 - u)
            expert(0)
            for f in range(OWN):
                give_back(0, f)

        return carry

    lax.fori_loop(first_late, Z, late_job, 0)

    ahead = min(AHEAD, U)
    for j in range(ahead):
        back_unit(U - 1 - j)

    def rs_copy(direction, u):
        return pltpu.make_async_remote_copy(
            src_ref=rs_out.at[direction, u],
            dst_ref=rs_in.at[direction, u],
            send_sem=rs_send.at[direction],
            recv_sem=rs_recv.at[direction, u],
            device_id=dev_z(1 if direction == 0 else -1),
            device_id_type=MESH,
        )

    for direction in range(2):
        for u in range(U, U + S):
            rs_in[direction, u] = jnp.zeros((T, DS), jnp.bfloat16)

    def gather_step(v, carry):
        u = U - 1 - v
        hop, i = u // S + 1, lax.rem(u, S)

        @pl.when(u >= ahead)
        def _():
            back_unit(u - ahead)

        @pl.when((v >= U - 3 - S - ahead) & (v < U - 1 - S - ahead))
        def _():
            expert(lax.rem((v - (U - 3 - S - ahead)) * 2 + Z - 1, Z))

        @pl.when(u == ahead - 1)
        def _():
            for f in range(OWN, S):
                give_back(0, f)

        for direction in (1, 0):
            o, f = (hop, S - 1 - i) if direction == 0 else (Z - hop, i)
            value = combine(o, f)

            @pl.when(u + S < U)
            def _():
                rs_copy(direction, u + S).wait_recv()

            value = value + rs_in[direction, u + S].astype(jnp.float32)
            rs_out[direction, u] = value.astype(jnp.bfloat16)
            rs_copy(direction, u).start()

        first = U // 2
        wide = att_ref.shape[1] // 4

        @pl.when(v == first)
        def _():
            bytes_wait(wall.at[pl.ds(0, X - 1)], w_recv)
            bytes_wait(hall.at[pl.ds(0, X - 1)], h_recv)

        @pl.when((v >= first) & (v < first + 4))
        def _():
            cut = pl.ds(pl.multiple_of((v - first) * wide, wide), wide)
            total = jnp.dot(hall[0], wall[0, :, cut], preferred_element_type=jnp.float32)
            for s in range(1, X):
                total += jnp.dot(hall[s], wall[s, :, cut], preferred_element_type=jnp.float32)
            att_ref[:, cut] = total.astype(jnp.bfloat16)

        return carry

    lax.fori_loop(0, U, gather_step, 0)

    for f in range(S):
        value = combine(0, f)
        rs_copy(0, S - 1 - f).wait_recv()
        rs_copy(1, f).wait_recv()
        value = value + rs_in[0, S - 1 - f].astype(jnp.float32) + rs_in[1, f].astype(jnp.float32)
        cut = slice(f * DS, (f + 1) * DS)
        out_ref[:, cut] = value.astype(jnp.bfloat16)

    bytes_wait(tab.at[pl.ds(0, Z - 1)], tab_send)
    for direction in range(2):
        bytes_wait(rs_in.at[direction, pl.ds(0, U)], z_send.at[direction])
        bytes_wait(rs_in.at[direction, pl.ds(0, U)], rs_send.at[direction])
    bytes_wait(disp.at[:, :, pl.ds(0, L - 1)], y_send)
    bytes_wait(res.at[:, :, pl.ds(0, L - 1)], r_send)
    bytes_wait(wall.at[pl.ds(0, X - 1)], w_send)
    bytes_wait(heads.at[pl.ds(0, X - 1)], h_send)
    halo.wait_send()


def on_device(
    Z,
    L,
    X,
    queries,
    head_keys,
    head_values,
    sink_logits,
    out_weight,
    moe_input,
    norm_gain,
    routes,
    route_weight,
    gate_weight,
    up_weight,
    down_weight,
):
    S = PIECES
    T, D = moe_input.shape
    DS = D // S
    FF = gate_weight.shape[2]
    rows, cols = queries.shape
    H = Z // 2
    U = (H - 1) * S + S // 2
    slots = L * CAP
    bf16, f32 = jnp.bfloat16, jnp.float32
    hbm = pl.BlockSpec(memory_space=pl.ANY)
    dma = pltpu.SemaphoreType.DMA
    attention_out, routed_out = pl.pallas_call(
        functools.partial(kernel, Z, L, X, S),
        out_shape=(
            pltpu.VMEM((rows // X, D), bf16),
            pltpu.VMEM((T, D), bf16),
        ),
        in_specs=[hbm] * 12,
        out_specs=(pl.BlockSpec(memory_space=pltpu.VMEM),) * 2,
        scratch_shapes=[
            pltpu.VMEM((T, D), bf16),
            pltpu.VMEM((1, D), f32),
            pltpu.VMEM(routes.shape[::-1], jnp.int32),
            pltpu.VMEM(routes.shape[::-1], f32),
            pltpu.VMEM((rows, cols), bf16),
            pltpu.VMEM((HEAD_DIM, rows), bf16),
            pltpu.VMEM((HEAD_DIM, rows), bf16),
            pltpu.SMEM(sink_logits.shape, f32),
            pltpu.VMEM((Z, S, T, DS), bf16),
            pltpu.VMEM((Z, 8, T), f32),
            pltpu.VMEM((Z, slots, T), bf16),
            pltpu.VMEM((Z, 2, T, slots), bf16),
            pltpu.VMEM((Z, S, L, CAP, DS), bf16),
            pltpu.VMEM((Z, S, L, CAP, DS), bf16),
            pltpu.VMEM((Z, S, L, CAP, DS), bf16),
            pltpu.VMEM((Z, S, L, CAP, DS), bf16),
            pltpu.VMEM((2, U, T, DS), bf16),
            pltpu.VMEM((2, U + S, T, DS), bf16),
            pltpu.VMEM((D, FF), bf16),
            pltpu.VMEM((D, FF), bf16),
            pltpu.VMEM((FF, D), bf16),
            pltpu.VMEM((X, cols, D), bf16),
            pltpu.VMEM((2, 2 * HEAD_DIM, rows + WINDOW), bf16),
            pltpu.VMEM((X, rows // X, cols), bf16),
            pltpu.VMEM((X, rows // X, cols), bf16),
            dma((12,)),
            dma,
            dma((Z,)),
            dma((2,)),
            dma((2, U)),
            dma,
            dma((Z,)),
            dma,
            dma((Z, S)),
            dma((2,)),
            dma((2, U)),
            dma,
            dma,
            dma,
            dma,
            dma,
            dma,
        ],
        compiler_params=pltpu.CompilerParams(
            collective_id=0, has_side_effects=True, vmem_limit_bytes=60 * 1024 * 1024
        ),
    )(
        moe_input,
        norm_gain.reshape(1, D),
        routes.T,
        route_weight.T,
        queries,
        head_keys.T,
        head_values.T,
        sink_logits,
        out_weight,
        gate_weight,
        up_weight,
        down_weight,
    )
    return write_out(attention_out, routed_out)


def write_out(*arrays):
    def body(*refs):
        copies = [pltpu.make_async_copy(refs[n], refs[2 + n], refs[4].at[n]) for n in range(2)]
        for copy in copies:
            copy.start()
        for copy in copies:
            copy.wait()

    return pl.pallas_call(
        body,
        out_shape=tuple(jax.ShapeDtypeStruct(a.shape, a.dtype) for a in arrays),
        in_specs=[pl.BlockSpec(memory_space=pltpu.VMEM)] * 2,
        out_specs=(pl.BlockSpec(memory_space=pl.ANY),) * 2,
        scratch_shapes=[pltpu.SemaphoreType.DMA((2,))],
    )(*[pltpu.with_memory_space_constraint(a, pltpu.VMEM) for a in arrays])


def solution(mesh, layer=8):
    X = mesh.shape["tp"]
    Z = mesh.shape["ep"] // layer
    placed = (
        P("ep", "tp"),
        P("ep", "tp"),
        P("ep", "tp"),
        P("tp"),
        P("tp", None),
        P(("ep", "tp"), None),
        P(),
        P(("ep", "tp"), None),
        P(("ep", "tp"), None),
        P("ep", None, None),
        P("ep", None, None),
        P("ep", None, None),
    )
    return jax.shard_map(
        functools.partial(on_device, Z, layer, X),
        mesh=mesh,
        in_specs=placed,
        out_specs=(P(("ep", "tp"), None), P(("ep", "tp"), None)),
        check_vma=False,
    )
```
